128 devices in a mesh: grp: 4 (over y, x), ep: 32 (over z, core).
Axes of the slice: x: 2, y: 2, z: 16, core: 2. Of those that a mesh axis runs over, the one named last changes fastest.
The devices are a block of a 8x8x16 slice.
Arguments:
- hidden: bfloat16 [384, 2048], P(('grp', 'ep')), parts along dimension 0, may hold values from -6 to 6
- conv_window: bfloat16 [384, 3, 6144], P(('grp', 'ep')), parts along dimension 0, may hold values from -6 to 6
- ssm_state: float32 [384, 64, 64, 128], P(('grp', 'ep')), parts along dimension 0, may hold values from -1.75 to 1.75
- gate_proj: bfloat16 [2048, 4096], P(None, 'ep'), may hold values from -0.125 to 0.125
- input_proj: bfloat16 [2048, 4096], P(None, 'ep'), may hold values from -0.125 to 0.125
- write_proj: bfloat16 [2048, 1024], P(None, 'ep'), may hold values from -0.125 to 0.125
- read_proj: bfloat16 [2048, 1024], P(None, 'ep'), may hold values from -0.125 to 0.125
- step_proj: bfloat16 [2048, 64], replicated, may hold values from -0.125 to 0.125
- step_bias: float32 [64], replicated, may hold values from -2 to 1
- decay_log: float32 [64], replicated, may hold values from -2.3 to 1.4
- decay_shift: float32 [384, 64], P(('grp', 'ep')), parts along dimension 0, may hold values from -0.7 to 0
- skip_scale: float32 [64], replicated, may hold values from -4 to 4
- conv_taps: bfloat16 [4, 6144], replicated, may hold values from -3 to 3
- conv_bias: float32 [6144], replicated, may hold values from -3 to 3
- mix_gain: float32 [2048], replicated, may hold values from 0.1 to 1.9
- group_gain: float32 [4096], replicated, may hold values from 0.1 to 1.9
- out_proj: bfloat16 [4096, 2048], P(None, 'ep'), may hold values from -0.09375 to 0.09375
- ffn_gain: float32 [2048], replicated, may hold values from 0.1 to 1.9
- router: bfloat16 [2048, 32], replicated, may hold values from -0.125 to 0.125
- expert_ids: int32 [384, 6], P(('grp', 'ep')), parts along dimension 0, may hold values from 0 to 31, all different within a row; in each aligned block of 3 rows (0 to 2, 3 to 5, ...) at most 2 rows name the same one
- expert_gate: bfloat16 [32, 2048, 512], P('ep'), may hold values from -0.125 to 0.125
- expert_up: bfloat16 [32, 2048, 512], P('ep'), may hold values from -0.125 to 0.125
- expert_down: bfloat16 [32, 512, 2048], P('ep'), may hold values from -0.25 to 0.25
- shared_gate: bfloat16 [2048, 512], P('ep'), may hold values from -0.125 to 0.125
- shared_up: bfloat16 [2048, 512], P('ep'), may hold values from -0.125 to 0.125
- shared_down: bfloat16 [512, 2048], replicated, may hold values from -0.25 to 0.25
Outputs:
- layer_out: bfloat16 [384, 2048], P(('grp', 'ep')), parts along dimension 0
- next_state: float32 [384, 64, 64, 128], P(('grp', 'ep')), parts along dimension 0
- next_window: bfloat16 [384, 3, 6144], P(('grp', 'ep')), parts along dimension 0
The draws below stay inside these ranges and needn't reach their ends.
There are 4 independent parts, one for each index of `grp`. The reference program is written for one: setup_inputs(seed, part) draws one part's arguments, and reference() takes and returns one part's arrays. A program takes and returns all parts, laid end to end along the dimension named above; an argument that names none is the same for every part. Nothing has to cross between parts.
Inputs may be any that keep to these rules, and one draw needn't show every extreme that they name: `expert_ids`: each row names 6 different experts; in the rows of one device no expert is named by more than 2 rows, and in every draw some device's rows name some expert exactly 2 times.
All inputs are finite; a program needn't handle non-finite values.
Results may differ from the reference program's by a relative error of at most 0.019.
Values may be sent and summed in bfloat16 or wider, within the bound.
A program may use at most 128 MiB of HBM per device.

```python
import math
import jax
import jax.numpy as jnp
import numpy as np
from jax import lax

D = 2048
INNER = 4096
HEAD_DIM = 64
GROUPS = 8
STATE = 128
CONV = 4
EFF = 512
SFF = 512
TOP_K = 6
SEQ_DEV = 3
CAP = 2
HEADS = 64
CONV_DIM = 6144
EXPERTS = 32
SEQS = 96


def block_levels(own_key, extent, shards, low, largest):
    loudness, own = 1.0, jax.random.fold_in(own_key, 6)
    for dim, shards_of in shards:
        draws = jnp.exp(jax.random.uniform(jax.random.fold_in(own, dim), (shards_of,), jnp.float32, low / len(shards), largest / len(shards)))
        loudness = loudness * jnp.repeat(draws, extent[dim] // shards_of).reshape([-1 if axis == dim else 1 for axis in range(len(extent))])
    return loudness


def routed_block(rng, own, number, rows, amount, top, limit, slope):
    order = jax.random.permutation(rng, amount)
    packed, ordinary = shares(amount, rows * top, limit, slope, True), shares(amount, rows * top, limit, slope, False)
    places = jnp.arange(amount)

    def named(lengths, offset_by):
        used = int((lengths > 0).sum())
        fixed = max(1, used // 4)
        passed = fixed + (places - fixed + offset_by * (used - fixed)) % max(1, amount - fixed)
        return jnp.zeros((amount,), jnp.int32).at[order[jnp.where(places < fixed, places, passed)]].set(jnp.asarray(lengths, jnp.int32))

    lengths = jnp.where(number % 4 == 0, named(packed, number // 4), named(ordinary, number - number // 4 - 1))
    mixed = jax.random.permutation(jax.random.fold_in(own, 3), amount)
    source_of, sink = mixed[0:amount // 2 * 2:2], mixed[1:amount // 2 * 2:2]
    slack = jnp.minimum(lengths[source_of] - 1, limit - lengths[sink]) // 2
    slack = jnp.where((source_of == order[0]) | (sink == order[0]) | (lengths[sink] == 0), 0, jnp.maximum(slack, 0))
    passed = jax.random.randint(jax.random.fold_in(own, 4), (amount // 2,), 0, 1 << 20) % (slack + 1)
    lengths = lengths.at[source_of].add(-passed).at[sink].add(passed)
    labels = jnp.searchsorted(jnp.cumsum(lengths), jnp.arange(rows * top), side="right").astype(jnp.int32)
    listing = labels.reshape(top, rows).T
    listing = listing[jax.random.permutation(jax.random.fold_in(own, 1), rows)]
    offset_by = jax.random.randint(jax.random.fold_in(own, 2), (rows, 1), 0, top)
    return jnp.take_along_axis(listing, (jnp.arange(top)[None, :] + offset_by) % top, axis=1)


def shares(count, total, most, lean, full):
    portions = [(1 << 20) // math.isqrt(grade ** lean) + 1 for grade in range(1, count + 1)]
    largest = most if full else min(most, max(-(-total // count), total * portions[0] // sum(portions)))
    least = 1 if total - largest >= count - 1 else 0
    given, rest = [largest] + [least] * (count - 1), total - largest - least * (count - 1)
    while rest > 0:
        free = [i for i in range(1, count) if given[i] < largest] or [i for i in range(1, count) if given[i] < most]
        pool, budget = sum([portions[i] for i in free]), rest
        for i in free:
            addition = min(most - given[i], max(1, budget * portions[i] // pool), rest)
            given[i] = given[i] + addition
            rest = rest - addition
    return np.array(given)


def gaussian(key, extent, deviation, most, pieces=(), held_as=jnp.bfloat16):
    values = deviation * jax.random.normal(key, extent, jnp.float32)
    if pieces:
        values = values * block_levels(key, extent, pieces, -0.22, 0.18)
    return jnp.clip(values, -most, most).astype(held_as)


def setup_inputs(seed: int = 0, part: int = 0) -> dict:
    seeds = jax.random.split(jax.random.key(seed), 27)
    part_keys = jax.random.split(jax.random.fold_in(seeds[26], part), 27)
    hidden = gaussian(part_keys[0], (SEQS, D), 1.0, 6.0, ((0, 32),))
    conv_window = gaussian(part_keys[1], (SEQS, CONV - 1, CONV_DIM), 1.0, 6.0, ((0, 32),))
    ssm_state = gaussian(part_keys[2], (SEQS, HEADS, HEAD_DIM, STATE), 0.3, 1.75, ((0, 32),), jnp.float32)
    gate_proj = gaussian(seeds[3], (D, INNER), D ** -0.5, 0.125, ((1, 32),))
    input_proj = gaussian(seeds[4], (D, INNER), D ** -0.5, 0.125, ((1, 32),))
    write_proj = gaussian(seeds[5], (D, GROUPS * STATE), D ** -0.5, 0.125, ((1, 32),))
    read_proj = gaussian(seeds[6], (D, GROUPS * STATE), D ** -0.5, 0.125, ((1, 32),))
    step_proj = gaussian(seeds[7], (D, HEADS), D ** -0.5, 0.125)
    step_bias = jnp.clip(jax.random.uniform(seeds[8], (HEADS,), jnp.float32, -2.0, 1.0), -2.0, 1.0)
    decay_log = jnp.clip(jax.random.uniform(seeds[9], (HEADS,), jnp.float32, -2.3, 1.4), -2.3, 1.4)
    decay_shift = jnp.clip(-0.7 + 0.7 * jax.random.uniform(part_keys[10], (SEQS, HEADS), jnp.float32) ** block_levels(part_keys[10], (SEQS, HEADS), ((0, 32),), -0.2, 0.2), -0.7, 0.0)
    skip_scale = gaussian(seeds[11], (HEADS,), 1.0, 4.0, (), jnp.float32)
    conv_taps = gaussian(seeds[12], (CONV, CONV_DIM), CONV ** -0.5, 3.0)
    conv_bias = gaussian(seeds[13], (CONV_DIM,), 0.5, 3.0, (), jnp.float32)
    mix_gain = jnp.clip(1.0 + 0.18 * jax.random.normal(seeds[14], (D,), jnp.float32), 0.1, 1.9)
    group_gain = jnp.clip(1.0 + 0.18 * jax.random.normal(seeds[15], (INNER,), jnp.float32), 0.1, 1.9)
    out_proj = gaussian(seeds[16], (INNER, D), INNER ** -0.5, 0.09375, ((1, 32),))
    ffn_gain = jnp.clip(1.0 + 0.18 * jax.random.normal(seeds[17], (D,), jnp.float32), 0.1, 1.9)
    router = gaussian(seeds[18], (D, EXPERTS), D ** -0.5, 0.125)
    expert_ids_keys = jax.random.split(jax.random.fold_in(part_keys[19], 1), SEQS // SEQ_DEV)
    expert_ids_turns = jax.random.permutation(jax.random.fold_in(part_keys[19], 3), SEQS // SEQ_DEV)
    expert_ids = jax.vmap(lambda own, number: routed_block(jax.random.fold_in(part_keys[19], 2), own, number, SEQ_DEV, EXPERTS, TOP_K, CAP, 2))(expert_ids_keys, expert_ids_turns).reshape((SEQS, TOP_K))
    expert_gate = gaussian(seeds[20], (EXPERTS, D, EFF), D ** -0.5, 0.125, ((0, 32),))
    expert_up = gaussian(seeds[21], (EXPERTS, D, EFF), D ** -0.5, 0.125, ((0, 32),))
    expert_down = gaussian(seeds[22], (EXPERTS, EFF, D), EFF ** -0.5, 0.25, ((0, 32),))
    shared_gate = gaussian(seeds[23], (D, SFF), D ** -0.5, 0.125, ((0, 32),))
    shared_up = gaussian(seeds[24], (D, SFF), D ** -0.5, 0.125, ((0, 32),))
    shared_down = gaussian(seeds[25], (SFF, D), SFF ** -0.5, 0.25)
    return {"hidden": hidden, "conv_window": conv_window, "ssm_state": ssm_state, "gate_proj": gate_proj, "input_proj": input_proj, "write_proj": write_proj, "read_proj": read_proj, "step_proj": step_proj, "step_bias": step_bias, "decay_log": decay_log, "decay_shift": decay_shift, "skip_scale": skip_scale, "conv_taps": conv_taps, "conv_bias": conv_bias, "mix_gain": mix_gain, "group_gain": group_gain, "out_proj": out_proj, "ffn_gain": ffn_gain, "router": router, "expert_ids": expert_ids, "expert_gate": expert_gate, "expert_up": expert_up, "expert_down": expert_down, "shared_gate": shared_gate, "shared_up": shared_up, "shared_down": shared_down}


epsilon = 1e-06
routed_scale = 2.5

def row_scale(values):
    return lax.rsqrt(lax.optimization_barrier(jnp.mean(values * values, axis=-1, keepdims=True)) + epsilon)

def matmul(left, right):
    return jnp.dot(left, right, preferred_element_type=jnp.float32)

def reference(hidden, conv_window, ssm_state, gate_proj, input_proj, write_proj, read_proj, step_proj, step_bias, decay_log, decay_shift, skip_scale, conv_taps, conv_bias, mix_gain, group_gain, out_proj, ffn_gain, router, expert_ids, expert_gate, expert_up, expert_down, shared_gate, shared_up, shared_down):
    batch_rows = hidden.shape[0]
    head_count = step_bias.shape[0]
    per_group = head_count // GROUPS
    inner_width = gate_proj.shape[1]
    state_span = GROUPS * STATE
    hidden_wide = hidden.astype(jnp.float32)
    normed = (hidden_wide * row_scale(hidden_wide) * mix_gain).astype(jnp.bfloat16)
    gate_rows = matmul(normed, gate_proj).astype(jnp.bfloat16)
    input_rows = matmul(normed, input_proj).astype(jnp.bfloat16)
    write_rows = matmul(normed, write_proj).astype(jnp.bfloat16)
    read_rows = matmul(normed, read_proj).astype(jnp.bfloat16)
    step_raw = matmul(normed, step_proj)
    fresh_row = jnp.concatenate([input_rows, write_rows, read_rows], axis=1)
    window = jnp.concatenate([conv_window, fresh_row[:, None, :]], axis=1)
    convolved = jax.nn.silu(lax.optimization_barrier(jnp.sum(window.astype(jnp.float32) * conv_taps.astype(jnp.float32)[None], axis=1)) + conv_bias)
    head_input = convolved[:, :inner_width].reshape(batch_rows, GROUPS, per_group, HEAD_DIM)
    write_vec = convolved[:, inner_width:inner_width + state_span].reshape(batch_rows, GROUPS, STATE)
    read_vec = convolved[:, inner_width + state_span:].reshape(batch_rows, GROUPS, STATE)
    step_size = jax.nn.softplus(step_raw + step_bias)
    decay_rate = jnp.exp(decay_shift - step_size * jnp.exp(decay_log)).reshape(batch_rows, GROUPS, per_group)
    step_group = step_size.reshape(batch_rows, GROUPS, per_group)
    carried = ssm_state.reshape(batch_rows, GROUPS, per_group, HEAD_DIM, STATE)
    next_state = decay_rate[..., None, None] * carried + (step_group[..., None] * head_input)[..., None] * write_vec[:, :, None, None, :]
    mixed_out = jnp.einsum('sgepn,sgn->sgep', next_state, read_vec, precision=lax.Precision.HIGHEST)
    mixed_out = mixed_out + skip_scale.reshape(GROUPS, per_group)[None, :, :, None] * head_input
    mixed_out = mixed_out.reshape(batch_rows, inner_width).astype(jnp.bfloat16)
    gated_out = mixed_out.astype(jnp.float32) * jax.nn.silu(gate_rows.astype(jnp.float32))
    blocks = gated_out.reshape(batch_rows, GROUPS, -1)
    gated_out = ((blocks * row_scale(blocks)).reshape(batch_rows, inner_width) * group_gain).astype(jnp.bfloat16)
    resid = (hidden_wide + matmul(gated_out, out_proj)).astype(jnp.bfloat16)
    resid_wide = resid.astype(jnp.float32)
    norm_scale = row_scale(resid_wide)
    routed_in = (resid_wide * norm_scale * ffn_gain).astype(jnp.bfloat16)
    shared_in = (resid_wide * ffn_gain).astype(jnp.bfloat16)
    scores = jax.nn.sigmoid(matmul(routed_in, router))
    picked = jnp.take_along_axis(scores, expert_ids, axis=1)
    weights = routed_scale * picked / lax.optimization_barrier(jnp.sum(picked, axis=1, keepdims=True))

    def add_expert(running, inputs):
        weight_gate, weight_up, weight_down, index = inputs
        expert_hidden = (jax.nn.silu(matmul(routed_in, weight_gate)) * matmul(routed_in, weight_up)).astype(jnp.bfloat16)
        result = matmul(expert_hidden, weight_down).astype(jnp.bfloat16)
        coefficient = lax.optimization_barrier(jnp.sum(jnp.where(expert_ids == index, weights, 0.0), axis=1))
        return (running + coefficient[:, None] * result.astype(jnp.float32), None)
    routed, _ = lax.scan(add_expert, jnp.zeros((batch_rows, hidden.shape[1]), jnp.float32), (expert_gate, expert_up, expert_down, jnp.arange(expert_gate.shape[0], dtype=jnp.int32)))
    shared_hidden = (jax.nn.silu(norm_scale * matmul(shared_in, shared_gate)) * (norm_scale * matmul(shared_in, shared_up))).astype(jnp.bfloat16)
    layer_out = (resid_wide + routed + matmul(shared_hidden, shared_down)).astype(jnp.bfloat16)
    return (layer_out, next_state.reshape(ssm_state.shape), window[:, 1:])
```

```python
import functools
import types

import jax
import jax.numpy as jnp
from jax import lax
from jax.experimental import pallas as pl
from jax.experimental.pallas import tpu as pltpu
from jax.sharding import PartitionSpec as P


MESH = pl.DeviceIdType.MESH
GRP_EP = ("grp", "ep")
F32, BF16 = jnp.float32, jnp.bfloat16
GROUPS, STATE, HEAD = 8, 128, 64
EPS = 1e-06
ROUTED_SCALE = 2.5

LEGS_HIDDEN = (8,)
LEGS_GATED = (4, 4)
LEGS_RESID = (8,)


def dot(a, b):
    return jnp.dot(a, b, preferred_element_type=F32)


def dot_nt(a, b):
    return lax.dot_general(a, b, (((1,), (1,)), ((), ())), preferred_element_type=F32)


def silu(v):
    return v * (1.0 / (1.0 + jnp.exp(-v)))


def lanes(tiles):
    return jnp.concatenate(tiles, axis=1)


def kernel(nz, rows, names, *refs):
    R = types.SimpleNamespace(**dict(zip(names, refs)))
    ep = lax.axis_index("ep")
    z, c = lax.div(ep, 2), lax.rem(ep, 2)
    half = nz // 2
    mine = rows * nz

    def ring(v):
        return lax.rem(v + nz, nz)

    def peer(zz):
        return {"ep": 2 * zz + c}

    partner = {"ep": 2 * z + 1 - c}

    barrier = pltpu.get_barrier_semaphore()

    def greet(d, _):
        pl.semaphore_signal(barrier, inc=1, device_id=peer(ring(z + d)), device_id_type=MESH)
        return 0

    lax.fori_loop(1, nz, greet, 0)
    pl.semaphore_signal(barrier, inc=1, device_id=partner, device_id_type=MESH)

    load_sem = R.load_sem
    handles = []

    def load(src, dst):
        copy = pltpu.make_async_copy(src, dst, load_sem.at[len(handles)])
        copy.start()
        handles.append(copy)
        return copy

    def ready(*copies):
        for copy in copies:
            copy.wait()

    L = types.SimpleNamespace()
    L.hidden = load(R.hidden, R.v_hidden)
    L.mgain = load(R.mgain, R.v_mgain)
    L.step_w = load(R.step_w, R.v_step_w)
    L.step_b = load(R.step_b, R.v_step_b)
    L.dlog = load(R.dlog, R.v_dlog)
    L.dshift = load(R.dshift, R.v_dshift)
    L.skip = load(R.skip, R.v_skip)
    L.ids = load(R.ids, R.v_ids)
    L.taps = load(R.taps, R.v_taps)
    L.cbias = load(R.cbias, R.v_cbias)
    L.window = load(R.window, R.v_window)
    L.ggain = load(R.ggain, R.v_ggain)
    L.fgain = load(R.fgain, R.v_fgain)
    L.gate = load(R.gate, R.wg.at[c])
    L.input = load(R.input, R.wi.at[c])
    L.write = load(R.write, R.wwr.at[c])
    L.read = load(R.read, R.wwr.at[2 + c])
    L.state = load(R.state, R.o_state)
    L.out_w = load(R.out_w, R.wo.at[c])
    L.router = load(R.router, R.v_router)
    L.s_gate = load(R.s_gate, R.sg.at[c])
    L.s_up = load(R.s_up, R.su.at[c])
    L.e_gate = load(R.e_gate.at[0], R.eg.at[c])
    L.e_up = load(R.e_up.at[0], R.eu.at[c])
    L.e_down = load(R.e_down.at[0], R.ed.at[c])
    L.s_down = load(R.s_down, R.v_s_down)

    S = types.SimpleNamespace()
    swapped = []

    def swap(src, dst):
        i = len(swapped)
        copy = pltpu.make_async_remote_copy(
            src_ref=src, dst_ref=dst, send_sem=R.swap_s.at[i], recv_sem=R.swap_r.at[i], device_id=partner, device_id_type=MESH
        )
        copy.start()
        swapped.append(copy)
        return copy

    def send(src, dst, ssem, rsem, zz):
        pltpu.make_async_remote_copy(
            src_ref=src, dst_ref=dst, send_sem=ssem, recv_sem=rsem, device_id=peer(zz), device_id_type=MESH
        ).start()

    def wait_recv(dst, ssem, rsem):
        pltpu.make_async_remote_copy(
            src_ref=dst, dst_ref=dst, send_sem=ssem, recv_sem=rsem, device_id=partner, device_id_type=MESH
        ).wait_recv()

    def wait_send(src, ssem, rsem):
        pltpu.make_async_remote_copy(
            src_ref=src, dst_ref=src, send_sem=ssem, recv_sem=rsem, device_id=partner, device_id_type=MESH
        ).wait_send()

    class Gather:
        def __init__(self, buf, ssem, rsem, legs):
            self.buf, self.ssem, self.rsem, self.legs, self.count = buf, ssem, rsem, legs, 0

        def one(self, block, zz):
            send(self.buf.at[block], self.buf.at[block], self.ssem.at[self.count], self.rsem.at[block], zz)
            self.count += 1

        def leg(self, done, length, block_of):
            for j in range(length, 0, -1):
                if done + j == half:
                    turn = 1 - 2 * c
                    self.one(block_of(turn), ring(z + turn * j))
                else:
                    for sign in (1, -1):
                        self.one(block_of(sign), ring(z + sign * j))

        def start(self):
            self.leg(0, self.legs[0], lambda sign: z)

        def finish(self, arrived):
            buf, done, seen = self.buf, self.legs[0], []

            def await_block(src):
                wait_recv(buf.at[src], self.ssem.at[0], self.rsem.at[src])

            for length in self.legs[1:]:
                for sign in (1, -1):
                    await_block(ring(z - sign * done))
                seen.append(done)
                at = done
                self.leg(done, length, lambda sign: ring(z - sign * at))
                done += length
            for distance in range(1, half + 1):
                for sign in (1, -1) if distance < half else (1,):
                    src = ring(z - sign * distance)
                    if distance not in seen:
                        await_block(src)
                    arrived(src)

        def drain(self):
            for i in range(self.count):
                wait_send(self.buf.at[0], self.ssem.at[i], self.rsem.at[0])

    def exchange(out, into, ssem, rsem):
        def body(i, _):
            k = lax.div(i + 1, 2)
            d = half + jnp.where(lax.rem(i, 2) == 1, -k, k)
            zz = ring(z + d)
            send(out.at[zz], into.at[z], ssem.at[i], rsem.at[z], zz)
            return 0

        lax.fori_loop(0, nz - 1, body, 0)
        into[z] = out[z]

    def collect(into, ssem, rsem, arrived, init=0):
        def body(d, carry):
            src = ring(z + d)
            wait_recv(into.at[src], ssem.at[0], rsem.at[src])
            return arrived(src, carry)

        return lax.fori_loop(1, nz, body, init)

    def drain(out, ssem, rsem):
        def body(i, _):
            wait_send(out.at[0], ssem.at[i], rsem.at[0])
            return 0

        lax.fori_loop(0, nz - 1, body, 0)

    ready(L.hidden, L.mgain)
    hid = R.v_hidden[...].astype(F32)
    depth = hid.shape[1]
    dt = depth // 128
    t1 = R.t1
    for s in range(dt):
        t1[pl.ds(s, rows, stride=dt), :] = hid[:, s * 128 : (s + 1) * 128]
    hbuf = R.hbuf
    hbuf[z] = t1[...].astype(BF16)
    pl.semaphore_wait(barrier, nz)
    g_hidden = Gather(hbuf, R.h_s, R.h_r, LEGS_HIDDEN)
    g_hidden.start()
    S.gate = swap(R.gate, R.wg.at[c])
    S.input = swap(R.input, R.wi.at[c])
    S.write = swap(R.write, R.wwr.at[c])
    S.read = swap(R.read, R.wwr.at[2 + c])
    S.out_w = swap(R.out_w, R.wo.at[c])
    S.s_gate = swap(R.s_gate, R.sg.at[c])
    S.s_up = swap(R.s_up, R.su.at[c])

    mgain = R.v_mgain[...]
    mrow = lanes([mgain[s : s + 1, :] for s in range(dt)])
    scale = lax.rsqrt(jnp.mean(hid * hid, axis=1, keepdims=True) + EPS)
    normed = (hid * scale * mrow).astype(BF16)
    ready(L.step_w, L.step_b, L.dlog, L.dshift, L.skip, L.ids, L.taps, L.cbias, L.window, L.ggain, L.fgain)
    pre = dot_nt(normed, R.v_step_w[...]) + R.v_step_b[...]
    step = jnp.maximum(pre, 0.0) + jnp.log1p(jnp.exp(-jnp.abs(pre)))
    decay = jnp.exp(R.v_dshift[...] - step * jnp.exp(R.v_dlog[...]))
    heads = decay.shape[1]
    t2 = R.t2
    t2[...] = jnp.zeros_like(t2)
    t2[0:rows, :] = decay
    t2[rows : 2 * rows, :] = step
    t2[2 * rows : 2 * rows + 1, :] = R.v_skip[...]
    per_head = t2[...]
    p_hi = per_head.astype(BF16)
    p_rest = per_head - p_hi.astype(F32)
    p_mid = p_rest.astype(BF16)
    p_lo = (p_rest - p_mid.astype(F32)).astype(BF16)
    span = heads // GROUPS * HEAD
    ex = R.ex
    for g in range(GROUPS):
        head_of = g * (heads // GROUPS) + lax.div(lax.broadcasted_iota(jnp.int32, (heads, span), 1), HEAD)
        spread = (head_of == lax.broadcasted_iota(jnp.int32, (heads, span), 0)).astype(F32).astype(BF16)
        ex[:, g * span : (g + 1) * span] = dot(p_hi, spread) + dot(p_mid, spread) + dot(p_lo, spread)
    eye = lax.broadcasted_iota(jnp.int32, (heads, heads), 0) == lax.broadcasted_iota(jnp.int32, (heads, heads), 1)
    for b in range(rows):
        column = jnp.sum(jnp.where(eye, decay[b : b + 1, :], 0.0), axis=1, keepdims=True)
        R.dcol[b] = jnp.broadcast_to(column, (heads, STATE))

    taps = R.v_taps[...].astype(F32)
    conv = R.conv
    for b in range(rows):
        past = R.v_window[b].astype(F32)
        conv[b : b + 1, :] = jnp.sum(past * taps[0:3, :], axis=0, keepdims=True) + R.v_cbias[...]
        R.nwf[b, 0:2, :] = past[1:3, :]

    ids = R.v_ids[...]
    lane3 = lax.broadcasted_iota(jnp.int32, (rows, 128), 1)
    slot3 = lax.broadcasted_iota(jnp.int32, (rows, 128), 0) * 32
    named = jnp.zeros((rows, 128), F32)
    for k in range(ids.shape[1]):
        named = named + jnp.where(lane3 == ids[:, k : k + 1] + slot3, 1.0, 0.0)
    named = jnp.sum(named, axis=0, keepdims=True)

    ready(L.state)
    o_state, sbf = R.o_state, R.sbf
    tiles = heads * HEAD // 128

    def cast_state(i, _):
        sbf[i] = o_state[i].astype(BF16)
        return 0

    lax.fori_loop(0, rows * tiles, cast_state, 0)

    f1 = R.f1

    def spread_hidden(src):
        for j in range(rows):
            at = pl.multiple_of(src * (rows * 24) + j * 24, 8)
            f1[pl.ds(at, dt), :] = hbuf[src, j * dt : (j + 1) * dt, :].astype(F32)

    spread_hidden(z)
    g_hidden.finish(spread_hidden)

    xs = [f1[pl.ds(s, mine, stride=24), :] for s in range(dt)]
    hcol = jnp.zeros_like(xs[0])
    total = jnp.zeros_like(xs[0])
    for s in range(dt):
        total = total + xs[s] * xs[s]
        hcol = jnp.where(z == s, xs[s], hcol)
    R.hcol[...] = hcol
    scale = lax.rsqrt(jnp.sum(total, axis=1, keepdims=True) / depth + EPS)
    x = R.x
    for s in range(dt):
        x[:, s * 128 : (s + 1) * 128] = (xs[s] * scale * mgain[s : s + 1, :]).astype(BF16)

    ready(L.gate, L.input, L.write, L.read)
    ready(S.gate, S.input, S.write, S.read)
    nx = x[...]
    prj = R.prj
    gates = dot(nx, lanes([R.wg[0], R.wg[1]]))
    inputs = dot(nx, lanes([R.wi[0], R.wi[1]]))
    prj[0], prj[1] = gates[:, :128], gates[:, 128:]
    prj[2], prj[3] = inputs[:, :128], inputs[:, 128:]
    wwr = R.wwr[...]
    prj[4] = dot_nt(nx, wwr.reshape(wwr.shape[0] * wwr.shape[1], wwr.shape[2]))
    m = R.m
    for t in range(5):
        for j in range(rows):
            m[pl.ds(3 * t + j, nz, stride=16), :] = prj[t, pl.ds(j, nz, stride=rows), :]
    m[pl.ds(15, nz, stride=16), :] = jnp.broadcast_to(named, (nz, 128))
    pout, pin = R.pout, R.pin
    for r in range(nz):
        pout[r] = m[16 * r : 16 * (r + 1), :].astype(BF16)
    exchange(pout, pin, R.p_s, R.p_r)
    S.e_gate = swap(R.e_gate.at[0], R.eg.at[c])
    S.e_up = swap(R.e_up.at[0], R.eu.at[c])
    S.e_down = swap(R.e_down.at[0], R.ed.at[c])
    g_hidden.drain()

    def spread_proj(src, carry):
        m[pl.ds(pl.multiple_of(src * 16, 16), 16), :] = pin[src].astype(F32)
        return carry

    spread_proj(z, 0)
    collect(pin, R.p_s, R.p_r, spread_proj)

    def tile(zz, t):
        return m[pl.ds(16 * zz + 3 * t, rows), :]

    gate_rows = lanes([tile(zz, t) for zz in range(nz) for t in (0, 1)])
    wr = [tile(zz, 4) for zz in range(nz)]
    low = lax.broadcasted_iota(jnp.int32, (rows, 128), 1) < 64
    rolled = [pltpu.roll(v, 64, 1) for v in wr]
    writes = [jnp.where(low, wr[2 * g], rolled[2 * g + 1]) for g in range(GROUPS)]
    reads = [jnp.where(low, rolled[2 * g], wr[2 * g + 1]) for g in range(GROUPS)]
    fresh = lanes([tile(zz, t) for zz in range(nz) for t in (2, 3)] + writes + reads)
    convolved = silu(conv[...] + fresh * taps[3:4, :])
    inner = heads * HEAD
    head_in = convolved[:, :inner]
    write = convolved[:, inner : inner + GROUPS * STATE]
    read = convolved[:, inner + GROUPS * STATE :]
    row_of = lax.broadcasted_iota(jnp.int32, (rows, STATE), 0)
    gated = []
    for g in range(GROUPS):
        rd = read[:, g * STATE : (g + 1) * STATE]
        wt = write[:, g * STATE : (g + 1) * STATE]
        acc = jnp.zeros((rows, span), F32)
        for b in range(rows):
            lhs = jnp.where(row_of == b, rd, 0.0).astype(BF16)
            first = (b * tiles) + g * (span // 128)
            held = sbf[first : first + span // 128]
            acc = acc + dot_nt(lhs, held.reshape(span, STATE))
        cut = slice(g * span, (g + 1) * span)
        hg = head_in[:, cut]
        inner_dot = jnp.sum(rd * wt, axis=1, keepdims=True)
        mixed = ex[0:rows, cut] * acc + (ex[rows : 2 * rows, cut] * inner_dot + ex[2 * rows : 2 * rows + 1, cut]) * hg
        mixed = mixed.astype(BF16).astype(F32) * silu(gate_rows[:, cut])
        mixed = mixed * lax.rsqrt(jnp.mean(mixed * mixed, axis=1, keepdims=True) + EPS)
        gated.append(mixed * R.v_ggain[:, cut])
    gated = lanes(gated)
    t3 = R.t3
    gt = inner // 128
    for k in range(gt):
        t3[pl.ds(k, rows, stride=gt), :] = gated[:, k * 128 : (k + 1) * 128]
    gbuf = R.gbuf
    gbuf[z] = t3[...].astype(BF16)
    g_gated = Gather(gbuf, R.g_s, R.g_r, LEGS_GATED)
    g_gated.start()

    drain(pout, R.p_s, R.p_r)
    masks = m[pl.ds(15, nz, stride=16), :]
    member = R.member
    for j in range(rows):
        member[pl.ds(j, nz, stride=rows), :] = pltpu.roll(masks, 128 - 32 * j, 1) if j else masks
    for b in range(rows):
        R.nwf[b, 2:3, :] = fresh[b : b + 1, :]
        R.o_window[b] = R.nwf[b].astype(BF16)
    u2, w2 = R.u2, R.w2
    u = ex[rows : 2 * rows, :] * head_in
    for k in range(gt):
        u2[pl.ds(k, rows, stride=gt), :] = u[:, k * 128 : (k + 1) * 128]
    for g in range(GROUPS):
        w2[pl.ds(g, rows, stride=GROUPS), :] = write[:, g * STATE : (g + 1) * STATE]
    f3 = R.f3

    def spread_gated(src):
        for j in range(rows):
            at = pl.multiple_of(src * (rows * 40) + j * 40, 8)
            f3[pl.ds(at, gt), :] = gbuf[src, j * gt : (j + 1) * gt, :].astype(F32)

    spread_gated(z)
    g_gated.finish(spread_gated)

    ready(L.out_w)
    ready(S.out_w)
    wo = R.wo[...]
    wo = wo.reshape(wo.shape[0] * wo.shape[1], wo.shape[2])
    a = R.a
    for k in range(gt):
        a[:, k * 128 : (k + 1) * 128] = f3[pl.ds(k, mine, stride=40), :].astype(BF16)
    rbuf = R.rbuf
    part = (R.hcol[...] + dot_nt(a[...], wo)).astype(BF16)
    rbuf[z] = part
    g_resid = Gather(rbuf, R.r_s, R.r_r, LEGS_RESID)
    g_resid.start()

    ready(L.s_gate, L.s_up)
    ready(S.s_gate)
    ready(S.s_up)
    shared_in = (part.astype(F32) * R.v_fgain[pl.ds(z, 1), :]).astype(BF16)
    sg, su = R.sg[...], R.su[...]
    sg = sg.reshape(sg.shape[0] * sg.shape[1], sg.shape[2])
    su = su.reshape(su.shape[0] * su.shape[1], su.shape[2])
    units = sg.shape[1]
    ut = units // 128
    pre_g, pre_u = dot(shared_in, sg), dot(shared_in, su)
    m6 = R.m6
    for k in range(ut):
        m6[pl.ds(k, mine, stride=2 * ut), :] = pre_g[:, k * 128 : (k + 1) * 128]
        m6[pl.ds(ut + k, mine, stride=2 * ut), :] = pre_u[:, k * 128 : (k + 1) * 128]
    qout, qin = R.qout, R.qin
    block = rows * 2 * ut
    for r in range(nz):
        qout[r] = m6[block * r : block * (r + 1), :].astype(BF16)
    exchange(qout, qin, R.q_s, R.q_r)

    eye2 = lax.broadcasted_iota(jnp.int32, (128, 128), 0) == lax.broadcasted_iota(jnp.int32, (128, 128), 1)

    def next_state(i, _):
        b, k = lax.div(i, tiles), lax.rem(i, tiles)
        column = jnp.sum(jnp.where(eye2, u2[pl.ds(i, 1), :], 0.0), axis=1, keepdims=True)
        fresh_part = column * w2[pl.ds(b * GROUPS + lax.div(k, tiles // GROUPS), 1), :]
        for hh in range(128 // HEAD):
            cut = slice(hh * HEAD, (hh + 1) * HEAD)
            keep = R.dcol[b, pl.ds((128 // HEAD) * k + hh, 1), :]
            o_state[i, cut, :] = o_state[i, cut, :] * keep + fresh_part[cut, :]
        return 0

    lax.fori_loop(0, rows * tiles, next_state, 0)
    g_gated.drain()
    g_resid.finish(lambda src: None)

    fgain = R.v_fgain[...]
    total = jnp.zeros((mine, 128), F32)
    for s in range(nz):
        v = rbuf[s].astype(F32)
        total = total + v * v
    scale = lax.rsqrt(jnp.sum(total, axis=1, keepdims=True) / depth + EPS)
    for s in range(nz):
        x[:, s * 128 : (s + 1) * 128] = (rbuf[s].astype(F32) * scale * fgain[s : s + 1, :]).astype(BF16)
    ready(L.router, L.e_gate, L.e_up, L.e_down)
    rx = x[...]
    experts = R.v_router.shape[0]
    logits = dot_nt(rx, R.v_router[...])
    chosen = member[...][:, :experts] / (1.0 + jnp.exp(-logits))
    weights = ROUTED_SCALE * chosen / jnp.sum(chosen, axis=1, keepdims=True)
    lane_e = lax.broadcasted_iota(jnp.int32, (mine, experts), 1)
    ready(S.e_gate, S.e_up, S.e_down)
    unit = R.eg.shape[2]
    hid_e = R.hid_e
    w_e = []
    for e in range(2):
        w_e.append(jnp.sum(jnp.where(lane_e == 2 * z + e, weights, 0.0), axis=1, keepdims=True))
        for n in range(0, unit, 256):
            up = dot(rx, R.eu[e, :, n : n + 256])
            hid_e[e, :, n : n + 256] = (silu(dot(rx, R.eg[e, :, n : n + 256])) * up).astype(BF16)
    m5 = R.m5
    for n in range(0, depth, 256):
        both = jnp.zeros((mine, 256), F32)
        for e in range(2):
            res = dot(hid_e[e], R.ed[e, :, n : n + 256]).astype(BF16).astype(F32)
            both = both + w_e[e] * res
        for i in range(2):
            m5[pl.ds(n // 128 + i, mine, stride=24), :] = both[:, i * 128 : (i + 1) * 128]
    cout, cin = R.cout, R.cin
    for r in range(nz):
        for j in range(rows):
            at = (rows * r + j) * 24
            cout[r, j * dt : (j + 1) * dt, :] = m5[at : at + dt, :].astype(BF16)
    exchange(cout, cin, R.c_s, R.c_r)

    first = lax.broadcasted_iota(jnp.int32, (8, mine), 0) + rows * z
    pick = (first == lax.broadcasted_iota(jnp.int32, (8, mine), 1)).astype(F32).astype(BF16)
    own = lanes([dot(pick, rbuf[s]) for s in range(nz)])[0:rows, :]
    scale = lax.rsqrt(jnp.mean(own * own, axis=1, keepdims=True) + EPS)
    t6 = R.t6
    t6[...] = collect(qin, R.q_s, R.q_r, lambda src, acc: acc + qin[src].astype(F32), qin[z].astype(F32))
    pre_g = lanes([t6[pl.ds(k, rows, stride=2 * ut), :] for k in range(ut)])
    pre_u = lanes([t6[pl.ds(ut + k, rows, stride=2 * ut), :] for k in range(ut)])
    shared_hidden = (silu(scale * pre_g) * (scale * pre_u)).astype(BF16)
    ready(L.s_down)
    own = own + dot(shared_hidden, R.v_s_down[...])
    g_resid.drain()
    drain(qout, R.q_s, R.q_r)
    t1[...] = collect(cin, R.c_s, R.c_r, lambda src, acc: acc + cin[src].astype(F32), cin[z].astype(F32))
    routed = lanes([t1[pl.ds(s, rows, stride=dt), :] for s in range(dt)])
    R.o_out[...] = (own + routed).astype(BF16)
    drain(cout, R.c_s, R.c_r)


def layer(
    nz, hidden, window, state, gate, input, write, read, step_w, step_b, dlog, dshift, skip, taps, cbias, mgain, ggain, out_w, fgain,
    router, ids, e_gate, e_up, e_down, s_gate, s_up, s_down
):
    A = types.SimpleNamespace(**locals())
    del A.nz
    inputs = tuple(vars(A))
    rows, depth = A.hidden.shape
    heads = A.step_b.shape[0]
    inner = heads * HEAD
    conv_dim = A.taps.shape[1]
    pre_rows = rows * 2 * A.s_gate.shape[1] // 128
    mine = rows * nz
    dt, gt = depth // 128, inner // 128
    state_shape = A.state.shape
    A.state = A.state.reshape(rows * gt, 128, STATE)
    A.write, A.read, A.step_w, A.out_w, A.router = A.write.T, A.read.T, A.step_w.T, A.out_w.T, A.router.T
    A.mgain, A.fgain = A.mgain.reshape(dt, 128), A.fgain.reshape(dt, 128)
    A.step_b, A.dlog, A.skip = A.step_b.reshape(1, heads), A.dlog.reshape(1, heads), A.skip.reshape(1, heads)
    A.cbias, A.ggain = A.cbias.reshape(1, conv_dim), A.ggain.reshape(1, inner)

    def like(array, *lead):
        return pltpu.VMEM((*lead, *array.shape), array.dtype)

    def f32(*shape):
        return pltpu.VMEM(shape, F32)

    def bf16(*shape):
        return pltpu.VMEM(shape, BF16)

    def sems(n):
        return pltpu.SemaphoreType.DMA((n,))

    scratch = dict(
        v_hidden=like(A.hidden), v_mgain=like(A.mgain), v_step_w=like(A.step_w), v_step_b=like(A.step_b), v_dlog=like(A.dlog),
        v_dshift=like(A.dshift), v_skip=like(A.skip), v_ids=like(A.ids), v_taps=like(A.taps), v_cbias=like(A.cbias),
        v_window=like(A.window), v_ggain=like(A.ggain), v_fgain=like(A.fgain), v_router=like(A.router), v_s_down=like(A.s_down),
        wg=like(A.gate, 2), wi=like(A.input, 2), wwr=like(A.write, 4), wo=like(A.out_w, 2), sg=like(A.s_gate, 2),
        su=like(A.s_up, 2), eg=like(A.e_gate[0], 2), eu=like(A.e_up[0], 2), ed=like(A.e_down[0], 2),
        t1=f32(rows * dt, 128), t2=f32(8, heads), t3=f32(rows * gt, 128), t6=f32(pre_rows, 128), ex=f32(8, inner),
        dcol=f32(rows, heads, STATE), conv=f32(rows, conv_dim), nwf=f32(rows, 3, conv_dim),
        sbf=bf16(rows * gt, 128, STATE), f1=f32(mine * 24, 128), f3=f32(mine * 40, 128), m5=f32(mine * 24, 128),
        m6=f32(nz * pre_rows, 128), hcol=f32(mine, 128), x=bf16(mine, depth), a=bf16(mine, inner), prj=f32(5, mine, 128),
        m=f32(nz * 16, 128), member=f32(mine, 128), u2=f32(rows * gt, 128), w2=f32(rows * GROUPS, 128),
        hid_e=bf16(2, mine, A.e_gate.shape[2]),
        hbuf=bf16(nz, rows * dt, 128), gbuf=bf16(nz, rows * gt, 128), rbuf=bf16(nz, mine, 128), pout=bf16(nz, 16, 128),
        pin=bf16(nz, 16, 128), qout=bf16(nz, pre_rows, 128), qin=bf16(nz, pre_rows, 128), cout=bf16(nz, rows * dt, 128),
        cin=bf16(nz, rows * dt, 128),
        load_sem=sems(32), swap_s=sems(10), swap_r=sems(10), h_s=sems(nz), h_r=sems(nz), p_s=sems(nz), p_r=sems(nz),
        g_s=sems(nz), g_r=sems(nz), r_s=sems(nz), r_r=sems(nz), q_s=sems(nz), q_r=sems(nz), c_s=sems(nz), c_r=sems(nz),
    )
    outs = dict(o_out=like(A.hidden), o_state=like(A.state), o_window=like(A.window))
    vm, anywhere = pl.BlockSpec(memory_space=pltpu.VMEM), pl.BlockSpec(memory_space=pl.ANY)
    made = pl.pallas_call(
        functools.partial(kernel, nz, rows, inputs + tuple(outs) + tuple(scratch)),
        out_shape=tuple(outs.values()),
        in_specs=[anywhere] * len(inputs),
        out_specs=(vm,) * 3,
        scratch_shapes=list(scratch.values()),
        compiler_params=pltpu.CompilerParams(collective_id=0, has_side_effects=True, vmem_limit_bytes=48 * 1024 * 1024),
        name="layer",
    )(*[getattr(A, name) for name in inputs])
    out, state, window = pl.pallas_call(
        write_out,
        out_shape=tuple(jax.ShapeDtypeStruct(v.shape, v.dtype) for v in made),
        in_specs=[vm] * 3,
        out_specs=(anywhere,) * 3,
        scratch_shapes=[sems(2 + PIECES)],
        compiler_params=pltpu.CompilerParams(vmem_limit_bytes=2**20),
        name="store",
    )(*[pltpu.with_memory_space_constraint(v, pltpu.VMEM) for v in made])
    return out, state.reshape(state_shape), window


PIECES = 4


def write_out(x, state, window, o_x, o_state, o_window, sem):
    copies = []
    step = state.shape[0] // PIECES
    for i in range(PIECES):
        copies.append(pltpu.make_async_copy(state.at[pl.ds(i * step, step)], o_state.at[pl.ds(i * step, step)], sem.at[i]))
    copies.append(pltpu.make_async_copy(x, o_x, sem.at[PIECES]))
    copies.append(pltpu.make_async_copy(window, o_window, sem.at[PIECES + 1]))
    for copy in copies:
        copy.start()
    for copy in copies:
        copy.wait()


def solution(mesh):
    nz = mesh.shape["ep"] // 2
    rows2, rows3, rows4 = P(GRP_EP, None), P(GRP_EP, None, None), P(GRP_EP, None, None, None)
    cols, lead, lead3 = P(None, "ep"), P("ep", None), P("ep", None, None)
    return jax.shard_map(
        functools.partial(layer, nz),
        mesh=mesh,
        in_specs=(
            rows2, rows3, rows4, cols, cols, cols, cols, P(), P(), P(), rows2, P(), P(), P(), P(), P(), cols, P(), P(), rows2,
            lead3, lead3, lead3, lead, lead, P(),
        ),
        out_specs=(rows2, rows4, rows3),
        check_vma=False,
    )
```

```python
import functools
import types

import jax
import jax.numpy as jnp
from jax import lax
from jax.experimental import pallas as pl
from jax.experimental.pallas import tpu as pltpu
from jax.sharding import PartitionSpec as P


MESH = pl.DeviceIdType.MESH
GRP_EP = ("grp", "ep")
F32, BF16 = jnp.float32, jnp.bfloat16
GROUPS, STATE, HEAD = 8, 128, 64
EPS = 1e-06
ROUTED_SCALE = 2.5

LEGS_HIDDEN = ((4, 4), (4, 4))
LEGS_GATED = ((4, 4), (2, 2, 2, 2))
LEGS_RESID = ((4, 4), (4, 4))
CUT_SHARED = (4, 4)
CUT_ROUTED = (4, 4)


def dot(a, b):
    return jnp.dot(a, b, preferred_element_type=F32)


def dot_nt(a, b):
    return lax.dot_general(a, b, (((1,), (1,)), ((), ())), preferred_element_type=F32)


def silu(v):
    return v * (1.0 / (1.0 + jnp.exp(-v)))


def lanes(tiles):
    return jnp.concatenate(tiles, axis=1)


def kernel(nz, rows, names, *refs):
    R = types.SimpleNamespace(**dict(zip(names, refs)))
    ep = lax.axis_index("ep")
    z, c = lax.div(ep, 2), lax.rem(ep, 2)
    half = nz // 2
    mine = rows * nz

    def ring(v):
        return lax.rem(v + nz, nz)

    def peer(zz):
        return {"ep": 2 * zz + c}

    partner = {"ep": 2 * z + 1 - c}

    load_sem = R.load_sem
    handles = []

    def load(src, dst):
        copy = pltpu.make_async_copy(src, dst, load_sem.at[len(handles)])
        copy.start()
        handles.append(copy)
        return copy

    def ready(*copies):
        for copy in copies:
            copy.wait()

    L = types.SimpleNamespace()
    L.hidden = load(R.hidden, R.v_hidden)
    L.mgain = load(R.mgain, R.v_mgain)

    def by_core(work):
        for core in (0, 1):
            pl.when(c == core)(functools.partial(work, core))

    barrier = pltpu.get_barrier_semaphore()

    def greet(d, _):
        pl.semaphore_signal(barrier, inc=1, device_id=peer(ring(z + d)), device_id_type=MESH)
        pl.semaphore_signal(barrier, inc=1, device_id=peer(ring(z - d)), device_id_type=MESH)
        return 0

    pl.semaphore_signal(barrier, inc=1, device_id=partner, device_id_type=MESH)
    near = max(LEGS_HIDDEN[0][0], LEGS_HIDDEN[1][0])
    lax.fori_loop(1, near + 1, greet, 0)

    S = types.SimpleNamespace()
    swapped = []

    def swap(src, dst):
        i = len(swapped)
        copy = pltpu.make_async_remote_copy(
            src_ref=src, dst_ref=dst, send_sem=R.swap_s.at[i], recv_sem=R.swap_r.at[i], device_id=partner, device_id_type=MESH
        )
        copy.start()
        swapped.append(copy)
        return copy

    def send(src, dst, ssem, rsem, zz):
        pltpu.make_async_remote_copy(
            src_ref=src, dst_ref=dst, send_sem=ssem, recv_sem=rsem, device_id=peer(zz), device_id_type=MESH
        ).start()

    def wait_recv(dst, ssem, rsem):
        pltpu.make_async_remote_copy(
            src_ref=dst, dst_ref=dst, send_sem=ssem, recv_sem=rsem, device_id=partner, device_id_type=MESH
        ).wait_recv()

    def wait_send(src, ssem, rsem):
        pltpu.make_async_remote_copy(
            src_ref=src, dst_ref=src, send_sem=ssem, recv_sem=rsem, device_id=partner, device_id_type=MESH
        ).wait_send()

    class Gather:
        def __init__(self, buf, ssem, rsem, legs, each):
            self.buf, self.ssem, self.rsem, self.legs, self.each = buf, ssem, rsem, legs, each
            self.last = rsem.shape[0] - 1

        def passed(self, core):
            legs = self.legs[core]
            return [sum(legs[: i + 1]) for i in range(len(legs) - 1)]

        def sem(self, core, sign, distance):
            if self.each:
                at = 2 * (distance - 1) + (sign < 0 and distance < half)
            elif distance in self.passed(core):
                at = 2 * self.passed(core).index(distance) + (sign < 0)
            else:
                at = self.last
            return self.rsem.at[at]

        def leg(self, core, done, length, block_of):
            for j in range(length, 0, -1):
                for sign in (1, -1) if done + j < half else (1 - 2 * core,):
                    block = block_of(sign)
                    to = self.buf.at[block]
                    send(to, to, self.ssem, self.sem(core, sign, done + j), ring(z + sign * j))

        def await_block(self, core, sign, distance):
            to = self.buf.at[ring(z - sign * distance)]
            wait_recv(to, self.ssem, self.sem(core, sign, distance))

        def start(self):
            by_core(lambda core: self.leg(core, 0, self.legs[core][0], lambda sign: z))

        def relay(self):
            def work(core):
                done = self.legs[core][0]
                for length in self.legs[core][1:]:
                    for sign in (1, -1):
                        self.await_block(core, sign, done)
                    self.leg(core, done, length, lambda sign: ring(z - sign * done))
                    done += length

            by_core(work)

        def finish(self):
            def work(core):
                rest = self.buf.at[pl.ds(0, nz - 1 - 2 * len(self.passed(core)))]
                wait_recv(rest, self.ssem, self.rsem.at[self.last])

            by_core(work)

        def drain(self):
            wait_send(self.buf.at[pl.ds(0, nz - 1)], self.ssem, self.rsem.at[0])

    def exchange(out, into, ssem, rsem):
        def body(i, _):
            k = lax.div(i + 1, 2)
            d = half + jnp.where(lax.rem(i, 2) == 1, -k, k)
            zz = ring(z + d)
            send(out.at[zz], into.at[z], ssem, rsem, zz)
            return 0

        lax.fori_loop(0, nz - 1, body, 0)

    def collect(into, ssem, rsem):
        wait_recv(into.at[pl.ds(0, nz - 1)], ssem, rsem)

    def drain(out, ssem, rsem):
        wait_send(out.at[pl.ds(0, nz - 1)], ssem, rsem)

    class Reduce:
        def __init__(self, out, mid, fin, sems, cuts):
            self.out, self.mid, self.fin, self.cuts = out, mid, fin, cuts
            self.ssem, self.fsem, self.msem = sems.at[0], sems.at[1], (sems.at[2], sems.at[3])

        def far(self, core, sign):
            cut = self.cuts[core]
            return half - cut - (sign != 1 - 2 * core)

        def slot(self, sign, j):
            return (half if sign < 0 else 0) + j - 1

        def start(self):
            def work(core):
                cut = self.cuts[core]
                if not cut:
                    exchange(self.out, self.fin, self.ssem, self.fsem)
                    return
                for j in range(half - cut, 0, -1):
                    for sign in (1, -1):
                        if j <= self.far(core, sign):
                            at = self.slot(sign, j)
                            src = self.out.at[ring(z + sign * (cut + j))]
                            send(src, self.mid.at[at], self.ssem, self.msem[sign < 0], ring(z + sign * j))
                for j in range(cut - 1, 0, -1):
                    for sign in (1, -1):
                        zz = ring(z + sign * j)
                        send(self.out.at[zz], self.fin.at[self.slot(sign, j)], self.ssem, self.fsem, zz)

            by_core(work)

        def relay(self):
            def work(core):
                cut = self.cuts[core]
                if not cut:
                    return
                for sign in (1, -1):
                    zz, many = ring(z + sign * cut), self.far(core, sign)
                    wait_recv(self.mid.at[pl.ds(self.slot(sign, 1), many)], self.ssem, self.msem[sign < 0])
                    terms = self.out[zz].astype(F32)
                    for j in range(1, many + 1):
                        terms = terms + self.mid[self.slot(sign, j)].astype(F32)
                    self.out[zz] = terms.astype(BF16)
                    send(self.out.at[zz], self.fin.at[self.slot(sign, cut)], self.ssem, self.fsem, zz)

            by_core(work)

        def finish(self, into):
            def work(core):
                cut = self.cuts[core]
                total = self.out[z].astype(F32)
                if cut:
                    wait_recv(self.fin.at[pl.ds(0, 2 * cut)], self.ssem, self.fsem)
                    for j in range(1, cut + 1):
                        for sign in (1, -1):
                            total = total + self.fin[self.slot(sign, j)].astype(F32)
                    into[...] = total
                else:
                    collect(self.fin, self.ssem, self.fsem)
                    into[...] = lax.fori_loop(1, nz, lambda d, acc: acc + self.fin[ring(z + d)].astype(F32), total)

            by_core(work)

        def drain(self):
            drain(self.out, self.ssem, self.fsem)

    ready(L.hidden, L.mgain)
    hid = R.v_hidden[...].astype(F32)
    depth = hid.shape[1]
    dt = depth // 128
    t1 = R.t1
    for s in range(dt):
        t1[pl.ds(s, rows, stride=dt), :] = hid[:, s * 128 : (s + 1) * 128]
    hbuf = R.hbuf
    hbuf[z] = t1[...].astype(BF16)
    pl.semaphore_wait(barrier, 2 * near + 1)
    g_hidden = Gather(hbuf, R.one.at[0], R.h_r, LEGS_HIDDEN, False)
    g_hidden.start()
    L.step_w = load(R.step_w, R.v_step_w)
    L.step_b = load(R.step_b, R.v_step_b)
    L.dlog = load(R.dlog, R.v_dlog)
    L.dshift = load(R.dshift, R.v_dshift)
    L.skip = load(R.skip, R.v_skip)
    L.ids = load(R.ids, R.v_ids)
    L.taps = load(R.taps, R.v_taps)
    L.cbias = load(R.cbias, R.v_cbias)
    L.window = load(R.window, R.v_window)
    L.ggain = load(R.ggain, R.v_ggain)
    L.fgain = load(R.fgain, R.v_fgain)
    L.gate = load(R.gate, R.wg.at[c])
    L.input = load(R.input, R.wi.at[c])
    L.write = load(R.write, R.wwr.at[c])
    L.read = load(R.read, R.wwr.at[2 + c])
    L.state = load(R.state, R.o_state)
    L.out_w = load(R.out_w, R.wo.at[c])
    L.router = load(R.router, R.v_router)
    L.s_gate = load(R.s_gate, R.sg.at[c])
    L.s_up = load(R.s_up, R.su.at[c])
    L.e_gate = load(R.e_gate.at[0], R.eg.at[c])
    L.e_up = load(R.e_up.at[0], R.eu.at[c])
    L.e_down = load(R.e_down.at[0], R.ed.at[c])
    L.s_down = load(R.s_down, R.v_s_down)
    S.gate = swap(R.gate, R.wg.at[c])
    S.input = swap(R.input, R.wi.at[c])
    S.write = swap(R.write, R.wwr.at[c])
    S.read = swap(R.read, R.wwr.at[2 + c])
    S.out_w = swap(R.out_w, R.wo.at[c])
    S.s_gate = swap(R.s_gate, R.sg.at[c])
    S.s_up = swap(R.s_up, R.su.at[c])

    mgain = R.v_mgain[...]
    mrow = lanes([mgain[s : s + 1, :] for s in range(dt)])
    scale = lax.rsqrt(jnp.mean(hid * hid, axis=1, keepdims=True) + EPS)
    normed = (hid * scale * mrow).astype(BF16)
    ready(L.step_w, L.step_b, L.dlog, L.dshift, L.skip, L.ids, L.taps, L.cbias, L.window, L.ggain, L.fgain)
    pre = dot_nt(normed, R.v_step_w[...]) + R.v_step_b[...]
    step = jnp.maximum(pre, 0.0) + jnp.log1p(jnp.exp(-jnp.abs(pre)))
    decay = jnp.exp(R.v_dshift[...] - step * jnp.exp(R.v_dlog[...]))
    heads = decay.shape[1]
    t2 = R.t2
    t2[...] = jnp.zeros_like(t2)
    t2[0:rows, :] = decay
    t2[rows : 2 * rows, :] = step
    t2[2 * rows : 2 * rows + 1, :] = R.v_skip[...]
    per_head = t2[...]
    p_hi = per_head.astype(BF16)
    p_rest = per_head - p_hi.astype(F32)
    p_mid = p_rest.astype(BF16)
    p_lo = (p_rest - p_mid.astype(F32)).astype(BF16)
    span = heads // GROUPS * HEAD
    ex = R.ex
    for g in range(GROUPS):
        head_of = g * (heads // GROUPS) + lax.div(lax.broadcasted_iota(jnp.int32, (heads, span), 1), HEAD)
        spread = (head_of == lax.broadcasted_iota(jnp.int32, (heads, span), 0)).astype(F32).astype(BF16)
        ex[:, g * span : (g + 1) * span] = dot(p_hi, spread) + dot(p_mid, spread) + dot(p_lo, spread)
    eye = lax.broadcasted_iota(jnp.int32, (heads, heads), 0) == lax.broadcasted_iota(jnp.int32, (heads, heads), 1)
    for b in range(rows):
        column = jnp.sum(jnp.where(eye, decay[b : b + 1, :], 0.0), axis=1, keepdims=True)
        R.dcol[b] = jnp.broadcast_to(column, (heads, STATE))

    g_hidden.relay()

    taps = R.v_taps[...].astype(F32)
    conv = R.conv
    for b in range(rows):
        past = R.v_window[b].astype(F32)
        conv[b : b + 1, :] = jnp.sum(past * taps[0:3, :], axis=0, keepdims=True) + R.v_cbias[...]
        R.nwf[b, 0:2, :] = past[1:3, :]

    ids = R.v_ids[...]
    lane3 = lax.broadcasted_iota(jnp.int32, (rows, 128), 1)
    slot3 = lax.broadcasted_iota(jnp.int32, (rows, 128), 0) * 32
    named = jnp.zeros((rows, 128), F32)
    for k in range(ids.shape[1]):
        named = named + jnp.where(lane3 == ids[:, k : k + 1] + slot3, 1.0, 0.0)
    named = jnp.sum(named, axis=0, keepdims=True)

    ready(L.state)
    o_state, sbf = R.o_state, R.sbf
    tiles = heads * HEAD // 128

    def cast_state(i, _):
        sbf[i] = o_state[i].astype(BF16)
        return 0

    lax.fori_loop(0, rows * tiles, cast_state, 0)

    f1 = R.f1

    def spread_hidden(src):
        for j in range(rows):
            at = src * (rows * 24) + j * 24
            f1[pl.ds(at, dt), :] = hbuf[src, j * dt : (j + 1) * dt, :].astype(F32)

    g_hidden.finish()
    for src in range(nz):
        spread_hidden(src)

    xs = [f1[pl.ds(s, mine, stride=24), :] for s in range(dt)]
    hcol = jnp.zeros_like(xs[0])
    total = jnp.zeros_like(xs[0])
    for s in range(dt):
        total = total + xs[s] * xs[s]
        hcol = jnp.where(z == s, xs[s], hcol)
    R.hcol[...] = hcol
    scale = lax.rsqrt(jnp.sum(total, axis=1, keepdims=True) / depth + EPS)
    x = R.x
    for s in range(dt):
        x[:, s * 128 : (s + 1) * 128] = (xs[s] * scale * mgain[s : s + 1, :]).astype(BF16)

    ready(L.gate, L.input, L.write, L.read)
    ready(S.gate, S.input, S.write, S.read)
    nx = x[...]
    prj = R.prj
    gates = dot(nx, lanes([R.wg[0], R.wg[1]]))
    inputs = dot(nx, lanes([R.wi[0], R.wi[1]]))
    prj[0], prj[1] = gates[:, :128], gates[:, 128:]
    prj[2], prj[3] = inputs[:, :128], inputs[:, 128:]
    wwr = R.wwr[...]
    prj[4] = dot_nt(nx, wwr.reshape(wwr.shape[0] * wwr.shape[1], wwr.shape[2]))
    m = R.m
    for t in range(5):
        for j in range(rows):
            m[pl.ds(3 * t + j, nz, stride=16), :] = prj[t, pl.ds(j, nz, stride=rows), :]
    m[pl.ds(15, nz, stride=16), :] = jnp.broadcast_to(named, (nz, 128))
    pout, pin = R.pout, R.pin
    for r in range(nz):
        pout[r] = m[16 * r : 16 * (r + 1), :].astype(BF16)
    exchange(pout, pin, R.one.at[3], R.one.at[4])
    pin[z] = pout[z]
    S.e_gate = swap(R.e_gate.at[0], R.eg.at[c])
    S.e_up = swap(R.e_up.at[0], R.eu.at[c])
    S.e_down = swap(R.e_down.at[0], R.ed.at[c])
    g_hidden.drain()

    collect(pin, R.one.at[3], R.one.at[4])
    for src in range(nz):
        m[src * 16 : (src + 1) * 16, :] = pin[src].astype(F32)

    def tile(zz, t):
        return m[pl.ds(16 * zz + 3 * t, rows), :]

    gate_rows = lanes([tile(zz, t) for zz in range(nz) for t in (0, 1)])
    wr = [tile(zz, 4) for zz in range(nz)]
    low = lax.broadcasted_iota(jnp.int32, (rows, 128), 1) < 64
    rolled = [pltpu.roll(v, 64, 1) for v in wr]
    writes = [jnp.where(low, wr[2 * g], rolled[2 * g + 1]) for g in range(GROUPS)]
    reads = [jnp.where(low, rolled[2 * g], wr[2 * g + 1]) for g in range(GROUPS)]
    fresh = lanes([tile(zz, t) for zz in range(nz) for t in (2, 3)] + writes + reads)
    convolved = silu(conv[...] + fresh * taps[3:4, :])
    inner = heads * HEAD
    head_in = convolved[:, :inner]
    write = convolved[:, inner : inner + GROUPS * STATE]
    read = convolved[:, inner + GROUPS * STATE :]
    row_of = lax.broadcasted_iota(jnp.int32, (rows, STATE), 0)
    gated = []
    for g in range(GROUPS):
        rd = read[:, g * STATE : (g + 1) * STATE]
        wt = write[:, g * STATE : (g + 1) * STATE]
        acc = jnp.zeros((rows, span), F32)
        for b in range(rows):
            lhs = jnp.where(row_of == b, rd, 0.0).astype(BF16)
            first = (b * tiles) + g * (span // 128)
            held = sbf[first : first + span // 128]
            acc = acc + dot_nt(lhs, held.reshape(span, STATE))
        cut = slice(g * span, (g + 1) * span)
        hg = head_in[:, cut]
        inner_dot = jnp.sum(rd * wt, axis=1, keepdims=True)
        mixed = ex[0:rows, cut] * acc + (ex[rows : 2 * rows, cut] * inner_dot + ex[2 * rows : 2 * rows + 1, cut]) * hg
        mixed = mixed.astype(BF16).astype(F32) * silu(gate_rows[:, cut])
        mixed = mixed * lax.rsqrt(jnp.mean(mixed * mixed, axis=1, keepdims=True) + EPS)
        gated.append(mixed * R.v_ggain[:, cut])
    gated = lanes(gated)
    t3 = R.t3
    gt = inner // 128
    for k in range(gt):
        t3[pl.ds(k, rows, stride=gt), :] = gated[:, k * 128 : (k + 1) * 128]
    gbuf = R.gbuf
    gbuf[z] = t3[...].astype(BF16)
    g_gated = Gather(gbuf, R.one.at[1], R.g_r, LEGS_GATED, False)
    g_gated.start()
    g_gated.relay()

    drain(pout, R.one.at[3], R.one.at[4])
    masks = m[pl.ds(15, nz, stride=16), :]
    member = R.member
    for j in range(rows):
        member[pl.ds(j, nz, stride=rows), :] = pltpu.roll(masks, 128 - 32 * j, 1) if j else masks
    for b in range(rows):
        R.nwf[b, 2:3, :] = fresh[b : b + 1, :]
        R.o_window[b] = R.nwf[b].astype(BF16)
    u2, w2 = R.u2, R.w2
    u = ex[rows : 2 * rows, :] * head_in
    for k in range(gt):
        u2[pl.ds(k, rows, stride=gt), :] = u[:, k * 128 : (k + 1) * 128]
    for g in range(GROUPS):
        w2[pl.ds(g, rows, stride=GROUPS), :] = write[:, g * STATE : (g + 1) * STATE]
    lane_t = lax.rem(lax.broadcasted_iota(jnp.int32, (1, 128), 1), tiles)

    def advance(b):
        u_b = u2[b * tiles : (b + 1) * tiles, :]
        u_hi = u_b.astype(BF16).astype(F32)
        flip = jnp.concatenate([u_hi, u_b - u_hi, u_hi, jnp.zeros((128 - 3 * tiles, 128), F32)], axis=0).T
        R.ut[b] = flip.astype(BF16)
        for g in range(GROUPS):
            per = tiles // GROUPS
            w_g = jnp.broadcast_to(w2[b * GROUPS + g : b * GROUPS + g + 1, :], (per, STATE))
            w_hi = w_g.astype(BF16).astype(F32)
            for part, v in enumerate((w_hi, w_hi, w_g - w_hi)):
                R.wt[b, part * tiles + g * per : part * tiles + (g + 1) * per, :] = v
        R.wt[b, 3 * tiles : 128, :] = jnp.zeros((128 - 3 * tiles, STATE), F32)
        base = R.ut[b].astype(F32)
        right = R.wt[b].astype(BF16)

        def next_state(k, _, b=b, base=base, right=right):
            fresh_part = dot(jnp.where(lane_t == k, base, 0.0).astype(BF16), right)
            i = b * tiles + k
            for hh in range(128 // HEAD):
                cut = slice(hh * HEAD, (hh + 1) * HEAD)
                keep = R.dcol[b, pl.ds((128 // HEAD) * k + hh, 1), :]
                o_state[i, cut, :] = o_state[i, cut, :] * keep + fresh_part[cut, :]
            return 0

        lax.fori_loop(0, tiles, next_state, 0, unroll=8)

    advance(0)
    f3 = R.f3

    def spread_gated(src):
        for j in range(rows):
            at = src * (rows * 40) + j * 40
            f3[pl.ds(at, gt), :] = gbuf[src, j * gt : (j + 1) * gt, :].astype(F32)

    g_gated.finish()
    for src in range(nz):
        spread_gated(src)

    ready(L.out_w)
    ready(S.out_w)
    wo = R.wo[...]
    wo = wo.reshape(wo.shape[0] * wo.shape[1], wo.shape[2])
    a = R.a
    for k in range(gt):
        a[:, k * 128 : (k + 1) * 128] = f3[pl.ds(k, mine, stride=40), :].astype(BF16)
    rbuf = R.rbuf
    part = (R.hcol[...] + dot_nt(a[...], wo)).astype(BF16)
    rbuf[z] = part
    g_resid = Gather(rbuf, R.one.at[2], R.r_r, LEGS_RESID, True)
    g_resid.start()

    ready(L.s_gate, L.s_up)
    ready(S.s_gate)
    ready(S.s_up)
    shared_in = (part.astype(F32) * R.v_fgain[pl.ds(z, 1), :]).astype(BF16)
    sg, su = R.sg[...], R.su[...]
    sg = sg.reshape(sg.shape[0] * sg.shape[1], sg.shape[2])
    su = su.reshape(su.shape[0] * su.shape[1], su.shape[2])
    units = sg.shape[1]
    ut = units // 128
    pre_g, pre_u = dot(shared_in, sg), dot(shared_in, su)
    m6 = R.m6
    for k in range(ut):
        m6[pl.ds(k, mine, stride=2 * ut), :] = pre_g[:, k * 128 : (k + 1) * 128]
        m6[pl.ds(ut + k, mine, stride=2 * ut), :] = pre_u[:, k * 128 : (k + 1) * 128]
    qout = R.qout
    block = rows * 2 * ut
    for r in range(nz):
        qout[r] = m6[block * r : block * (r + 1), :].astype(BF16)
    g_resid.relay()
    sum_q = Reduce(qout, R.qmid, R.qfin, R.q_sem, CUT_SHARED)

    for b in range(1, rows):
        advance(b)
    g_gated.drain()

    ready(L.router, L.e_gate, L.e_up, L.e_down)
    ready(S.e_gate, S.e_up, S.e_down)
    experts, unit = R.v_router.shape[0], R.eg.shape[2]
    squares, logits, pre = R.squares, R.logits, R.pre
    squares[...] = jnp.zeros_like(squares)
    logits[...] = jnp.zeros_like(logits)
    pre[...] = jnp.zeros_like(pre)

    def features(src):
        v = rbuf[src].astype(F32)
        squares[...] += v * v
        v = (v * R.v_fgain[pl.ds(src, 1), :]).astype(BF16)
        cut = pl.ds(pl.multiple_of(src * 128, 128), 128)
        logits[...] += dot_nt(v, R.v_router[:, cut])
        for e in range(2):
            pre[2 * e] += dot(v, R.eg[e, cut, :])
            pre[2 * e + 1] += dot(v, R.eu[e, cut, :])

    features(z)

    def take(core):
        for distance in range(1, half + 1):
            for sign in (1, -1) if distance < half else (1 - 2 * core,):
                if distance not in g_resid.passed(core):
                    g_resid.await_block(core, sign, distance)
                features(ring(z - sign * distance))

    by_core(take)
    sum_q.start()
    scale = lax.rsqrt(jnp.sum(squares[...], axis=1, keepdims=True) / depth + EPS)
    chosen = member[...][:, :experts] / (1.0 + jnp.exp(-scale * logits[...]))
    weights = ROUTED_SCALE * chosen / jnp.sum(chosen, axis=1, keepdims=True)
    lane_e = lax.broadcasted_iota(jnp.int32, (mine, experts), 1)
    hid_e = R.hid_e
    w_e = []
    for e in range(2):
        w_e.append(jnp.sum(jnp.where(lane_e == 2 * z + e, weights, 0.0), axis=1, keepdims=True))
        hid_e[e] = (silu(scale * pre[2 * e]) * (scale * pre[2 * e + 1])).astype(BF16)
    m5 = R.m5
    for n in range(0, depth, 256):
        both = jnp.zeros((mine, 256), F32)
        for e in range(2):
            res = dot(hid_e[e], R.ed[e, :, n : n + 256]).astype(BF16).astype(F32)
            both = both + w_e[e] * res
        for i in range(2):
            m5[pl.ds(n // 128 + i, mine, stride=24), :] = both[:, i * 128 : (i + 1) * 128]
    cout = R.cout
    for r in range(nz):
        for j in range(rows):
            at = (rows * r + j) * 24
            cout[r, j * dt : (j + 1) * dt, :] = m5[at : at + dt, :].astype(BF16)
    sum_c = Reduce(cout, R.cmid, R.cfin, R.c_sem, CUT_ROUTED)
    sum_c.start()
    sum_q.relay()
    sum_c.relay()

    first = lax.broadcasted_iota(jnp.int32, (8, mine), 0) + rows * z
    pick = (first == lax.broadcasted_iota(jnp.int32, (8, mine), 1)).astype(F32).astype(BF16)
    own = lanes([dot(pick, rbuf[s]) for s in range(nz)])[0:rows, :]
    scale = lax.rsqrt(jnp.mean(own * own, axis=1, keepdims=True) + EPS)
    t6 = R.t6
    sum_q.finish(t6)
    pre_g = lanes([t6[pl.ds(k, rows, stride=2 * ut), :] for k in range(ut)])
    pre_u = lanes([t6[pl.ds(ut + k, rows, stride=2 * ut), :] for k in range(ut)])
    shared_hidden = (silu(scale * pre_g) * (scale * pre_u)).astype(BF16)
    ready(L.s_down)
    own = own + dot(shared_hidden, R.v_s_down[...])
    g_resid.drain()
    sum_q.drain()
    sum_c.finish(t1)
    routed = lanes([t1[pl.ds(s, rows, stride=dt), :] for s in range(dt)])
    R.o_out[...] = (own + routed).astype(BF16)
    sum_c.drain()


def layer(
    nz, hidden, window, state, gate, input, write, read, step_w, step_b, dlog, dshift, skip, taps, cbias, mgain, ggain, out_w, fgain,
    router, ids, e_gate, e_up, e_down, s_gate, s_up, s_down
):
    A = types.SimpleNamespace(**locals())
    del A.nz
    inputs = tuple(vars(A))
    rows, depth = A.hidden.shape
    heads = A.step_b.shape[0]
    inner = heads * HEAD
    conv_dim = A.taps.shape[1]
    pre_rows = rows * 2 * A.s_gate.shape[1] // 128
    mine = rows * nz
    dt, gt = depth // 128, inner // 128
    state_shape = A.state.shape
    A.state = A.state.reshape(rows * gt, 128, STATE)
    A.write, A.read, A.step_w, A.out_w, A.router = A.write.T, A.read.T, A.step_w.T, A.out_w.T, A.router.T
    A.mgain, A.fgain = A.mgain.reshape(dt, 128), A.fgain.reshape(dt, 128)
    A.step_b, A.dlog, A.skip = A.step_b.reshape(1, heads), A.dlog.reshape(1, heads), A.skip.reshape(1, heads)
    A.cbias, A.ggain = A.cbias.reshape(1, conv_dim), A.ggain.reshape(1, inner)

    def like(array, *lead):
        return pltpu.VMEM((*lead, *array.shape), array.dtype)

    def f32(*shape):
        return pltpu.VMEM(shape, F32)

    def bf16(*shape):
        return pltpu.VMEM(shape, BF16)

    def sems(n):
        return pltpu.SemaphoreType.DMA((n,))

    scratch = dict(
        v_hidden=like(A.hidden), v_mgain=like(A.mgain), v_step_w=like(A.step_w), v_step_b=like(A.step_b), v_dlog=like(A.dlog),
        v_dshift=like(A.dshift), v_skip=like(A.skip), v_ids=like(A.ids), v_taps=like(A.taps), v_cbias=like(A.cbias),
        v_window=like(A.window), v_ggain=like(A.ggain), v_fgain=like(A.fgain), v_router=like(A.router), v_s_down=like(A.s_down),
        wg=like(A.gate, 2), wi=like(A.input, 2), wwr=like(A.write, 4), wo=like(A.out_w, 2), sg=like(A.s_gate, 2),
        su=like(A.s_up, 2), eg=like(A.e_gate[0], 2), eu=like(A.e_up[0], 2), ed=like(A.e_down[0], 2),
        t1=f32(rows * dt, 128), t2=f32(8, heads), t3=f32(rows * gt, 128), t6=f32(pre_rows, 128), ex=f32(8, inner),
        dcol=f32(rows, heads, STATE), conv=f32(rows, conv_dim), nwf=f32(rows, 3, conv_dim),
        sbf=bf16(rows * gt, 128, STATE), f1=f32(mine * 24, 128), f3=f32(mine * 40, 128), m5=f32(mine * 24, 128),
        m6=f32(nz * pre_rows, 128), hcol=f32(mine, 128), ut=bf16(rows, 128, 128), wt=f32(rows, 128, STATE), x=bf16(mine, depth), a=bf16(mine, inner), prj=f32(5, mine, 128),
        m=f32(nz * 16, 128), member=f32(mine, 128), u2=f32(rows * gt, 128), w2=f32(rows * GROUPS, 128),
        hid_e=bf16(2, mine, A.e_gate.shape[2]), squares=f32(mine, 128), logits=f32(mine, A.router.shape[0]),
        pre=f32(4, mine, A.e_gate.shape[2]),
        hbuf=bf16(nz, rows * dt, 128), gbuf=bf16(nz, rows * gt, 128), rbuf=bf16(nz, mine, 128), pout=bf16(nz, 16, 128),
        pin=bf16(nz, 16, 128), qout=bf16(nz, pre_rows, 128), qmid=bf16(nz, pre_rows, 128), qfin=bf16(nz, pre_rows, 128), cout=bf16(nz, rows * dt, 128),
        cmid=bf16(nz, rows * dt, 128), cfin=bf16(nz, rows * dt, 128),
        load_sem=sems(26), swap_s=sems(10), swap_r=sems(10), h_r=sems(3), g_r=sems(7), r_r=sems(nz - 1), one=sems(5), q_sem=sems(4), c_sem=sems(4),
    )
    outs = dict(o_out=like(A.hidden), o_state=like(A.state), o_window=like(A.window))
    vm, anywhere = pl.BlockSpec(memory_space=pltpu.VMEM), pl.BlockSpec(memory_space=pl.ANY)
    made = pl.pallas_call(
        functools.partial(kernel, nz, rows, inputs + tuple(outs) + tuple(scratch)),
        out_shape=tuple(outs.values()),
        in_specs=[anywhere] * len(inputs),
        out_specs=(vm,) * 3,
        scratch_shapes=list(scratch.values()),
        compiler_params=pltpu.CompilerParams(collective_id=0, has_side_effects=True, vmem_limit_bytes=48 * 1024 * 1024),
        name="layer",
    )(*[getattr(A, name) for name in inputs])
    out, state, window = pl.pallas_call(
        write_out,
        out_shape=tuple(jax.ShapeDtypeStruct(v.shape, v.dtype) for v in made),
        in_specs=[vm] * 3,
        out_specs=(anywhere,) * 3,
        scratch_shapes=[sems(2 + PIECES)],
        compiler_params=pltpu.CompilerParams(vmem_limit_bytes=2**20),
        name="store",
    )(*[pltpu.with_memory_space_constraint(v, pltpu.VMEM) for v in made])
    return out, state.reshape(state_shape), window


PIECES = 4


def write_out(x, state, window, o_x, o_state, o_window, sem):
    copies = []
    step = state.shape[0] // PIECES
    for i in range(PIECES):
        copies.append(pltpu.make_async_copy(state.at[pl.ds(i * step, step)], o_state.at[pl.ds(i * step, step)], sem.at[i]))
    copies.append(pltpu.make_async_copy(x, o_x, sem.at[PIECES]))
    copies.append(pltpu.make_async_copy(window, o_window, sem.at[PIECES + 1]))
    for copy in copies:
        copy.start()
    for copy in copies:
        copy.wait()


def solution(mesh):
    nz = mesh.shape["ep"] // 2
    rows2, rows3, rows4 = P(GRP_EP, None), P(GRP_EP, None, None), P(GRP_EP, None, None, None)
    cols, lead, lead3 = P(None, "ep"), P("ep", None), P("ep", None, None)
    return jax.shard_map(
        functools.partial(layer, nz),
        mesh=mesh,
        in_specs=(
            rows2, rows3, rows4, cols, cols, cols, cols, P(), P(), P(), rows2, P(), P(), P(), P(), P(), cols, P(), P(), rows2,
            lead3, lead3, lead3, lead, lead, P(),
        ),
        out_specs=(rows2, rows4, rows3),
        check_vma=False,
    )
```

```python
import functools
import types

import jax
import jax.numpy as jnp
from jax import lax
from jax.experimental import pallas as pl
from jax.experimental.pallas import tpu as pltpu
from jax.sharding import PartitionSpec as P


MESH = pl.DeviceIdType.MESH
GRP_EP = ("grp", "ep")
F32, BF16 = jnp.float32, jnp.bfloat16
GROUPS, STATE, HEAD = 8, 128, 64
EPS = 1e-06
ROUTED_SCALE = 2.5

LEGS_HIDDEN = ((4, 4), (4, 4))
LEGS_GATED = ((4, 4), (2, 2, 2, 2))
LEGS_RESID = ((4, 4), (4, 4))
CUT_SHARED = (4, 4)
CUT_ROUTED = (4, 4)


def dot(a, b):
    return jnp.dot(a, b, preferred_element_type=F32)


def dot_nt(a, b):
    return lax.dot_general(a, b, (((1,), (1,)), ((), ())), preferred_element_type=F32)


def silu(v):
    return 0.5 * v * (1.0 + jnp.tanh(0.5 * v))


def lanes(tiles):
    return jnp.concatenate(tiles, axis=1)


def kernel(nz, rows, names, *refs):
    R = types.SimpleNamespace(**dict(zip(names, refs)))
    ep = lax.axis_index("ep")
    z, c = lax.div(ep, 2), lax.rem(ep, 2)
    half = nz // 2
    mine = rows * nz

    def ring(v):
        return lax.rem(v + nz, nz)

    def peer(zz):
        return {"ep": 2 * zz + c}

    partner = {"ep": 2 * z + 1 - c}

    load_sem = R.load_sem
    handles = []

    def load(src, dst):
        copy = pltpu.make_async_copy(src, dst, load_sem.at[len(handles)])
        copy.start()
        handles.append(copy)
        return copy

    def ready(*copies):
        for copy in copies:
            copy.wait()

    L = types.SimpleNamespace()
    L.hidden = load(R.hidden, R.v_hidden)
    L.mgain = load(R.mgain, R.v_mgain)

    def by_core(work):
        for core in (0, 1):
            pl.when(c == core)(functools.partial(work, core))

    barrier = pltpu.get_barrier_semaphore()

    def greet(d, _):
        pl.semaphore_signal(barrier, inc=1, device_id=peer(ring(z + d)), device_id_type=MESH)
        pl.semaphore_signal(barrier, inc=1, device_id=peer(ring(z - d)), device_id_type=MESH)
        return 0

    pl.semaphore_signal(barrier, inc=1, device_id=partner, device_id_type=MESH)
    near = max(LEGS_HIDDEN[0][0], LEGS_HIDDEN[1][0])
    lax.fori_loop(1, near + 1, greet, 0)

    S = types.SimpleNamespace()
    swapped = []

    def swap(src, dst):
        i = len(swapped)
        copy = pltpu.make_async_remote_copy(
            src_ref=src, dst_ref=dst, send_sem=R.swap_s.at[i], recv_sem=R.swap_r.at[i], device_id=partner, device_id_type=MESH
        )
        copy.start()
        swapped.append(copy)
        return copy

    def send(src, dst, ssem, rsem, zz):
        pltpu.make_async_remote_copy(
            src_ref=src, dst_ref=dst, send_sem=ssem, recv_sem=rsem, device_id=peer(zz), device_id_type=MESH
        ).start()

    def wait_recv(dst, ssem, rsem):
        pltpu.make_async_remote_copy(
            src_ref=dst, dst_ref=dst, send_sem=ssem, recv_sem=rsem, device_id=partner, device_id_type=MESH
        ).wait_recv()

    def wait_send(src, ssem, rsem):
        pltpu.make_async_remote_copy(
            src_ref=src, dst_ref=src, send_sem=ssem, recv_sem=rsem, device_id=partner, device_id_type=MESH
        ).wait_send()

    class Gather:
        def __init__(self, buf, ssem, rsem, legs, each):
            self.buf, self.ssem, self.rsem, self.legs, self.each = buf, ssem, rsem, legs, each
            self.last = rsem.shape[0] - 1

        def passed(self, core):
            legs = self.legs[core]
            return [sum(legs[: i + 1]) for i in range(len(legs) - 1)]

        def sem(self, core, sign, distance):
            if self.each:
                at = 2 * (distance - 1) + (sign < 0 and distance < half)
            elif distance in self.passed(core):
                at = 2 * self.passed(core).index(distance) + (sign < 0)
            else:
                at = self.last
            return self.rsem.at[at]

        def leg(self, core, done, length, block_of):
            for j in range(length, 0, -1):
                for sign in (1, -1) if done + j < half else (1 - 2 * core,):
                    block = block_of(sign)
                    to = self.buf.at[block]
                    send(to, to, self.ssem, self.sem(core, sign, done + j), ring(z + sign * j))

        def await_block(self, core, sign, distance):
            to = self.buf.at[ring(z - sign * distance)]
            wait_recv(to, self.ssem, self.sem(core, sign, distance))

        def start(self):
            by_core(lambda core: self.leg(core, 0, self.legs[core][0], lambda sign: z))

        def relay(self):
            def work(core):
                done = self.legs[core][0]
                for length in self.legs[core][1:]:
                    for sign in (1, -1):
                        self.await_block(core, sign, done)
                    self.leg(core, done, length, lambda sign: ring(z - sign * done))
                    done += length

            by_core(work)

        def finish(self):
            def work(core):
                rest = self.buf.at[pl.ds(0, nz - 1 - 2 * len(self.passed(core)))]
                wait_recv(rest, self.ssem, self.rsem.at[self.last])

            by_core(work)

        def drain(self):
            wait_send(self.buf.at[pl.ds(0, nz - 1)], self.ssem, self.rsem.at[0])

    def exchange(out, into, ssem, rsem):
        def body(i, _):
            k = lax.div(i + 1, 2)
            d = half + jnp.where(lax.rem(i, 2) == 1, -k, k)
            zz = ring(z + d)
            send(out.at[zz], into.at[z], ssem, rsem, zz)
            return 0

        lax.fori_loop(0, nz - 1, body, 0)

    def collect(into, ssem, rsem):
        wait_recv(into.at[pl.ds(0, nz - 1)], ssem, rsem)

    def drain(out, ssem, rsem):
        wait_send(out.at[pl.ds(0, nz - 1)], ssem, rsem)

    class Reduce:
        def __init__(self, out, mid, fin, sems, cuts):
            self.out, self.mid, self.fin, self.cuts = out, mid, fin, cuts
            self.ssem, self.fsem, self.msem = sems.at[0], sems.at[1], (sems.at[2], sems.at[3])

        def far(self, core, sign):
            cut = self.cuts[core]
            return half - cut - (sign != 1 - 2 * core)

        def slot(self, sign, j):
            return (half if sign < 0 else 0) + j - 1

        def start(self):
            def work(core):
                cut = self.cuts[core]
                if not cut:
                    exchange(self.out, self.fin, self.ssem, self.fsem)
                    return
                for j in range(half - cut, 0, -1):
                    for sign in (1, -1):
                        if j <= self.far(core, sign):
                            at = self.slot(sign, j)
                            src = self.out.at[ring(z + sign * (cut + j))]
                            send(src, self.mid.at[at], self.ssem, self.msem[sign < 0], ring(z + sign * j))
                for j in range(cut - 1, 0, -1):
                    for sign in (1, -1):
                        zz = ring(z + sign * j)
                        send(self.out.at[zz], self.fin.at[self.slot(sign, j)], self.ssem, self.fsem, zz)

            by_core(work)

        def relay(self):
            def work(core):
                cut = self.cuts[core]
                if not cut:
                    return
                for sign in (1, -1):
                    zz, many = ring(z + sign * cut), self.far(core, sign)
                    wait_recv(self.mid.at[pl.ds(self.slot(sign, 1), many)], self.ssem, self.msem[sign < 0])
                    terms = self.out[zz].astype(F32)
                    for j in range(1, many + 1):
                        terms = terms + self.mid[self.slot(sign, j)].astype(F32)
                    self.out[zz] = terms.astype(BF16)
                    send(self.out.at[zz], self.fin.at[self.slot(sign, cut)], self.ssem, self.fsem, zz)

            by_core(work)

        def finish(self, into):
            def work(core):
                cut = self.cuts[core]
                total = self.out[z].astype(F32)
                if cut:
                    wait_recv(self.fin.at[pl.ds(0, 2 * cut)], self.ssem, self.fsem)
                    for j in range(1, cut + 1):
                        for sign in (1, -1):
                            total = total + self.fin[self.slot(sign, j)].astype(F32)
                    into[...] = total
                else:
                    collect(self.fin, self.ssem, self.fsem)
                    into[...] = lax.fori_loop(1, nz, lambda d, acc: acc + self.fin[ring(z + d)].astype(F32), total)

            by_core(work)

        def drain(self):
            drain(self.out, self.ssem, self.fsem)

    ready(L.hidden, L.mgain)
    hid = R.v_hidden[...].astype(F32)
    depth = hid.shape[1]
    dt = depth // 128
    t1 = R.t1
    for s in range(dt):
        t1[pl.ds(s, rows, stride=dt), :] = hid[:, s * 128 : (s + 1) * 128]
    hbuf = R.hbuf
    hbuf[z] = t1[...].astype(BF16)
    pl.semaphore_wait(barrier, 2 * near + 1)
    g_hidden = Gather(hbuf, R.one.at[0], R.h_r, LEGS_HIDDEN, False)
    g_hidden.start()
    L.step_w = load(R.step_w, R.v_step_w)
    L.step_b = load(R.step_b, R.v_step_b)
    L.dlog = load(R.dlog, R.v_dlog)
    L.dshift = load(R.dshift, R.v_dshift)
    L.skip = load(R.skip, R.v_skip)
    L.ids = load(R.ids, R.v_ids)
    L.taps = load(R.taps, R.v_taps)
    L.cbias = load(R.cbias, R.v_cbias)
    L.window = load(R.window, R.v_window)
    L.ggain = load(R.ggain, R.v_ggain)
    L.fgain = load(R.fgain, R.v_fgain)
    L.gate = load(R.gate, R.wg.at[c])
    L.input = load(R.input, R.wi.at[c])
    L.write = load(R.write, R.wwr.at[c])
    L.read = load(R.read, R.wwr.at[2 + c])
    L.state = load(R.state, R.o_state)
    L.out_w = load(R.out_w, R.wo.at[c])
    L.router = load(R.router, R.v_router)
    L.s_gate = load(R.s_gate, R.sg.at[c])
    L.s_up = load(R.s_up, R.su.at[c])
    L.e_gate = load(R.e_gate.at[0], R.eg.at[c])
    L.e_up = load(R.e_up.at[0], R.eu.at[c])
    L.e_down = load(R.e_down.at[0], R.ed.at[c])
    L.s_down = load(R.s_down, R.v_s_down)
    S.gate = swap(R.gate, R.wg.at[c])
    S.input = swap(R.input, R.wi.at[c])
    S.write = swap(R.write, R.wwr.at[c])
    S.read = swap(R.read, R.wwr.at[2 + c])
    S.out_w = swap(R.out_w, R.wo.at[c])
    S.s_gate = swap(R.s_gate, R.sg.at[c])
    S.s_up = swap(R.s_up, R.su.at[c])

    mgain = R.v_mgain[...]
    mrow = lanes([mgain[s : s + 1, :] for s in range(dt)])
    scale = lax.rsqrt(jnp.mean(hid * hid, axis=1, keepdims=True) + EPS)
    normed = (hid * scale * mrow).astype(BF16)
    ready(L.step_w, L.step_b, L.dlog, L.dshift, L.skip, L.ids, L.taps, L.cbias, L.window, L.ggain, L.fgain)
    pre = dot_nt(normed, R.v_step_w[...]) + R.v_step_b[...]
    step = jnp.maximum(pre, 0.0) + jnp.log1p(jnp.exp(-jnp.abs(pre)))
    decay = jnp.exp(R.v_dshift[...] - step * jnp.exp(R.v_dlog[...]))
    heads = decay.shape[1]
    t2 = R.t2
    t2[...] = jnp.zeros_like(t2)
    t2[0:rows, :] = decay
    t2[rows : 2 * rows, :] = step
    t2[2 * rows : 2 * rows + 1, :] = R.v_skip[...]
    per_head = t2[...]
    p_hi = per_head.astype(BF16)
    p_rest = per_head - p_hi.astype(F32)
    p_mid = p_rest.astype(BF16)
    p_lo = (p_rest - p_mid.astype(F32)).astype(BF16)
    span = heads // GROUPS * HEAD
    ex = R.ex
    for g in range(GROUPS):
        head_of = g * (heads // GROUPS) + lax.div(lax.broadcasted_iota(jnp.int32, (heads, span), 1), HEAD)
        spread = (head_of == lax.broadcasted_iota(jnp.int32, (heads, span), 0)).astype(F32).astype(BF16)
        ex[:, g * span : (g + 1) * span] = dot(p_hi, spread) + dot(p_mid, spread) + dot(p_lo, spread)
    eye = lax.broadcasted_iota(jnp.int32, (heads, heads), 0) == lax.broadcasted_iota(jnp.int32, (heads, heads), 1)
    for b in range(rows):
        column = jnp.sum(jnp.where(eye, decay[b : b + 1, :], 0.0), axis=1, keepdims=True)
        R.dcol[b] = jnp.broadcast_to(column, (heads, STATE))

    g_hidden.relay()

    taps = R.v_taps[...].astype(F32)
    conv = R.conv
    for b in range(rows):
        past = R.v_window[b].astype(F32)
        conv[b : b + 1, :] = jnp.sum(past * taps[0:3, :], axis=0, keepdims=True) + R.v_cbias[...]
        R.nwf[b, 0:2, :] = past[1:3, :]

    ids = R.v_ids[...]
    lane3 = lax.broadcasted_iota(jnp.int32, (rows, 128), 1)
    slot3 = lax.broadcasted_iota(jnp.int32, (rows, 128), 0) * 32
    named = jnp.zeros((rows, 128), F32)
    for k in range(ids.shape[1]):
        named = named + jnp.where(lane3 == ids[:, k : k + 1] + slot3, 1.0, 0.0)
    named = jnp.sum(named, axis=0, keepdims=True)

    ready(L.state)
    o_state, sbf = R.o_state, R.sbf
    tiles = heads * HEAD // 128

    def cast_state(i, _):
        sbf[i] = o_state[i].astype(BF16)
        return 0

    lax.fori_loop(0, rows * tiles, cast_state, 0)

    f1 = R.f1

    def spread_hidden(src):
        for j in range(rows):
            at = src * (rows * 24) + j * 24
            f1[pl.ds(at, dt), :] = hbuf[src, j * dt : (j + 1) * dt, :].astype(F32)

    g_hidden.finish()
    for src in range(nz):
        spread_hidden(src)

    xs = [f1[pl.ds(s, mine, stride=24), :] for s in range(dt)]
    hcol = jnp.zeros_like(xs[0])
    total = jnp.zeros_like(xs[0])
    for s in range(dt):
        total = total + xs[s] * xs[s]
        hcol = jnp.where(z == s, xs[s], hcol)
    R.hcol[...] = hcol
    scale = lax.rsqrt(jnp.sum(total, axis=1, keepdims=True) / depth + EPS)
    x = R.x
    for s in range(dt):
        x[:, s * 128 : (s + 1) * 128] = (xs[s] * scale * mgain[s : s + 1, :]).astype(BF16)

    ready(L.gate, L.input, L.write, L.read)
    ready(S.gate, S.input, S.write, S.read)
    nx = x[...]
    prj = R.prj
    gates = dot(nx, lanes([R.wg[0], R.wg[1]]))
    inputs = dot(nx, lanes([R.wi[0], R.wi[1]]))
    prj[0], prj[1] = gates[:, :128], gates[:, 128:]
    prj[2], prj[3] = inputs[:, :128], inputs[:, 128:]
    wwr = R.wwr[...]
    prj[4] = dot_nt(nx, wwr.reshape(wwr.shape[0] * wwr.shape[1], wwr.shape[2]))
    m = R.m
    for t in range(5):
        for j in range(rows):
            m[pl.ds(3 * t + j, nz, stride=16), :] = prj[t, pl.ds(j, nz, stride=rows), :]
    m[pl.ds(15, nz, stride=16), :] = jnp.broadcast_to(named, (nz, 128))
    pout, pin = R.pout, R.pin
    for r in range(nz):
        pout[r] = m[16 * r : 16 * (r + 1), :].astype(BF16)
    exchange(pout, pin, R.one.at[3], R.one.at[4])
    pin[z] = pout[z]
    S.e_gate = swap(R.e_gate.at[0], R.eg.at[c])
    S.e_up = swap(R.e_up.at[0], R.eu.at[c])
    S.e_down = swap(R.e_down.at[0], R.ed.at[c])
    g_hidden.drain()

    collect(pin, R.one.at[3], R.one.at[4])
    for src in range(nz):
        m[src * 16 : (src + 1) * 16, :] = pin[src].astype(F32)

    def tile(zz, t):
        return m[pl.ds(16 * zz + 3 * t, rows), :]

    gate_rows = lanes([tile(zz, t) for zz in range(nz) for t in (0, 1)])
    wr = [tile(zz, 4) for zz in range(nz)]
    low = lax.broadcasted_iota(jnp.int32, (rows, 128), 1) < 64
    rolled = [pltpu.roll(v, 64, 1) for v in wr]
    writes = [jnp.where(low, wr[2 * g], rolled[2 * g + 1]) for g in range(GROUPS)]
    reads = [jnp.where(low, rolled[2 * g], wr[2 * g + 1]) for g in range(GROUPS)]
    fresh = lanes([tile(zz, t) for zz in range(nz) for t in (2, 3)] + writes + reads)
    convolved = silu(conv[...] + fresh * taps[3:4, :])
    inner = heads * HEAD
    head_in = convolved[:, :inner]
    write = convolved[:, inner : inner + GROUPS * STATE]
    read = convolved[:, inner + GROUPS * STATE :]
    row_of = lax.broadcasted_iota(jnp.int32, (rows, STATE), 0)
    gated = []
    for g in range(GROUPS):
        rd = read[:, g * STATE : (g + 1) * STATE]
        wt = write[:, g * STATE : (g + 1) * STATE]
        acc = jnp.zeros((rows, span), F32)
        for b in range(rows):
            lhs = jnp.where(row_of == b, rd, 0.0).astype(BF16)
            first = (b * tiles) + g * (span // 128)
            held = sbf[first : first + span // 128]
            acc = acc + dot_nt(lhs, held.reshape(span, STATE))
        cut = slice(g * span, (g + 1) * span)
        hg = head_in[:, cut]
        inner_dot = jnp.sum(rd * wt, axis=1, keepdims=True)
        mixed = ex[0:rows, cut] * acc + (ex[rows : 2 * rows, cut] * inner_dot + ex[2 * rows : 2 * rows + 1, cut]) * hg
        mixed = mixed.astype(BF16).astype(F32) * silu(gate_rows[:, cut])
        mixed = mixed * lax.rsqrt(jnp.mean(mixed * mixed, axis=1, keepdims=True) + EPS)
        gated.append(mixed * R.v_ggain[:, cut])
    gated = lanes(gated)
    t3 = R.t3
    gt = inner // 128
    for k in range(gt):
        t3[pl.ds(k, rows, stride=gt), :] = gated[:, k * 128 : (k + 1) * 128]
    gbuf = R.gbuf
    gbuf[z] = t3[...].astype(BF16)
    g_gated = Gather(gbuf, R.one.at[1], R.g_r, LEGS_GATED, False)
    g_gated.start()
    g_gated.relay()

    drain(pout, R.one.at[3], R.one.at[4])
    masks = m[pl.ds(15, nz, stride=16), :]
    member = R.member
    for j in range(rows):
        member[pl.ds(j, nz, stride=rows), :] = pltpu.roll(masks, 128 - 32 * j, 1) if j else masks
    for b in range(rows):
        R.nwf[b, 2:3, :] = fresh[b : b + 1, :]
        R.o_window[b] = R.nwf[b].astype(BF16)
    u2, w2 = R.u2, R.w2
    u = ex[rows : 2 * rows, :] * head_in
    for k in range(gt):
        u2[pl.ds(k, rows, stride=gt), :] = u[:, k * 128 : (k + 1) * 128]
    for g in range(GROUPS):
        w2[pl.ds(g, rows, stride=GROUPS), :] = write[:, g * STATE : (g + 1) * STATE]
    lane_t = lax.rem(lax.broadcasted_iota(jnp.int32, (1, 128), 1), tiles)

    def advance(b):
        u_b = u2[b * tiles : (b + 1) * tiles, :]
        u_hi = u_b.astype(BF16).astype(F32)
        flip = jnp.concatenate([u_hi, u_b - u_hi, u_hi, jnp.zeros((128 - 3 * tiles, 128), F32)], axis=0).T
        R.ut[b] = flip.astype(BF16)
        for g in range(GROUPS):
            per = tiles // GROUPS
            w_g = jnp.broadcast_to(w2[b * GROUPS + g : b * GROUPS + g + 1, :], (per, STATE))
            w_hi = w_g.astype(BF16).astype(F32)
            for part, v in enumerate((w_hi, w_hi, w_g - w_hi)):
                R.wt[b, part * tiles + g * per : part * tiles + (g + 1) * per, :] = v
        R.wt[b, 3 * tiles : 128, :] = jnp.zeros((128 - 3 * tiles, STATE), F32)
        base = R.ut[b].astype(F32)
        right = R.wt[b].astype(BF16)

        def next_state(k, _, b=b, base=base, right=right):
            fresh_part = dot(jnp.where(lane_t == k, base, 0.0).astype(BF16), right)
            i = b * tiles + k
            for hh in range(128 // HEAD):
                cut = slice(hh * HEAD, (hh + 1) * HEAD)
                keep = R.dcol[b, pl.ds((128 // HEAD) * k + hh, 1), :]
                o_state[i, cut, :] = o_state[i, cut, :] * keep + fresh_part[cut, :]
            return 0

        lax.fori_loop(0, tiles, next_state, 0, unroll=8)

    advance(0)
    f3 = R.f3

    def spread_gated(src):
        for j in range(rows):
            at = src * (rows * 40) + j * 40
            f3[pl.ds(at, gt), :] = gbuf[src, j * gt : (j + 1) * gt, :].astype(F32)

    g_gated.finish()
    for src in range(nz):
        spread_gated(src)

    ready(L.out_w)
    ready(S.out_w)
    wo = R.wo[...]
    wo = wo.reshape(wo.shape[0] * wo.shape[1], wo.shape[2])
    a = R.a
    for k in range(gt):
        a[:, k * 128 : (k + 1) * 128] = f3[pl.ds(k, mine, stride=40), :].astype(BF16)
    rbuf = R.rbuf
    part = (R.hcol[...] + dot_nt(a[...], wo)).astype(BF16)
    rbuf[z] = part
    g_resid = Gather(rbuf, R.one.at[2], R.r_r, LEGS_RESID, True)
    g_resid.start()

    ready(L.s_gate, L.s_up)
    ready(S.s_gate)
    ready(S.s_up)
    shared_in = (part.astype(F32) * R.v_fgain[pl.ds(z, 1), :]).astype(BF16)
    sg, su = R.sg[...], R.su[...]
    sg = sg.reshape(sg.shape[0] * sg.shape[1], sg.shape[2])
    su = su.reshape(su.shape[0] * su.shape[1], su.shape[2])
    units = sg.shape[1]
    ut = units // 128
    pre_g, pre_u = dot(shared_in, sg), dot(shared_in, su)
    m6 = R.m6
    for k in range(ut):
        m6[pl.ds(k, mine, stride=2 * ut), :] = pre_g[:, k * 128 : (k + 1) * 128]
        m6[pl.ds(ut + k, mine, stride=2 * ut), :] = pre_u[:, k * 128 : (k + 1) * 128]
    qout = R.qout
    block = rows * 2 * ut
    for r in range(nz):
        qout[r] = m6[block * r : block * (r + 1), :].astype(BF16)
    g_resid.relay()
    sum_q = Reduce(qout, R.qmid, R.qfin, R.q_sem, CUT_SHARED)

    for b in range(1, rows):
        advance(b)
    g_gated.drain()

    ready(L.router, L.e_gate, L.e_up, L.e_down)
    ready(S.e_gate, S.e_up, S.e_down)
    experts, unit = R.v_router.shape[0], R.eg.shape[2]
    squares, logits, pre = R.squares, R.logits, R.pre
    squares[...] = jnp.zeros_like(squares)
    logits[...] = jnp.zeros_like(logits)
    pre[...] = jnp.zeros_like(pre)

    def features(src):
        v = rbuf[src].astype(F32)
        squares[...] += v * v
        v = (v * R.v_fgain[pl.ds(src, 1), :]).astype(BF16)
        cut = pl.ds(pl.multiple_of(src * 128, 128), 128)
        logits[...] += dot_nt(v, R.v_router[:, cut])
        for e in range(2):
            pre[2 * e] += dot(v, R.eg[e, cut, :])
            pre[2 * e + 1] += dot(v, R.eu[e, cut, :])

    features(z)

    def take(core):
        for distance in range(1, half + 1):
            for sign in (1, -1) if distance < half else (1 - 2 * core,):
                if distance not in g_resid.passed(core):
                    g_resid.await_block(core, sign, distance)
                features(ring(z - sign * distance))

    by_core(take)
    sum_q.start()
    scale = lax.rsqrt(jnp.sum(squares[...], axis=1, keepdims=True) / depth + EPS)
    chosen = member[...][:, :experts] / (1.0 + jnp.exp(-scale * logits[...]))
    weights = ROUTED_SCALE * chosen / jnp.sum(chosen, axis=1, keepdims=True)
    lane_e = lax.broadcasted_iota(jnp.int32, (mine, experts), 1)
    hid_e = R.hid_e
    w_e = []
    for e in range(2):
        w_e.append(jnp.sum(jnp.where(lane_e == 2 * z + e, weights, 0.0), axis=1, keepdims=True))
        hid_e[e] = (silu(scale * pre[2 * e]) * (scale * pre[2 * e + 1])).astype(BF16)
    m5 = R.m5
    for n in range(0, depth, 256):
        both = jnp.zeros((mine, 256), F32)
        for e in range(2):
            res = dot(hid_e[e], R.ed[e, :, n : n + 256]).astype(BF16).astype(F32)
            both = both + w_e[e] * res
        for i in range(2):
            m5[pl.ds(n // 128 + i, mine, stride=24), :] = both[:, i * 128 : (i + 1) * 128]
    cout = R.cout
    for r in range(nz):
        for j in range(rows):
            at = (rows * r + j) * 24
            cout[r, j * dt : (j + 1) * dt, :] = m5[at : at + dt, :].astype(BF16)
    sum_c = Reduce(cout, R.cmid, R.cfin, R.c_sem, CUT_ROUTED)
    sum_c.start()
    sum_q.relay()
    sum_c.relay()

    first = lax.broadcasted_iota(jnp.int32, (8, mine), 0) + rows * z
    pick = (first == lax.broadcasted_iota(jnp.int32, (8, mine), 1)).astype(F32).astype(BF16)
    own = lanes([dot(pick, rbuf[s]) for s in range(nz)])[0:rows, :]
    scale = lax.rsqrt(jnp.mean(own * own, axis=1, keepdims=True) + EPS)
    t6 = R.t6
    sum_q.finish(t6)
    pre_g = lanes([t6[pl.ds(k, rows, stride=2 * ut), :] for k in range(ut)])
    pre_u = lanes([t6[pl.ds(ut + k, rows, stride=2 * ut), :] for k in range(ut)])
    shared_hidden = (silu(scale * pre_g) * (scale * pre_u)).astype(BF16)
    ready(L.s_down)
    own = own + dot(shared_hidden, R.v_s_down[...])
    g_resid.drain()
    sum_q.drain()
    sum_c.finish(t1)
    routed = lanes([t1[pl.ds(s, rows, stride=dt), :] for s in range(dt)])
    R.o_out[...] = (own + routed).astype(BF16)
    sum_c.drain()


def layer(
    nz, hidden, window, state, gate, input, write, read, step_w, step_b, dlog, dshift, skip, taps, cbias, mgain, ggain, out_w, fgain,
    router, ids, e_gate, e_up, e_down, s_gate, s_up, s_down
):
    A = types.SimpleNamespace(**locals())
    del A.nz
    inputs = tuple(vars(A))
    rows, depth = A.hidden.shape
    heads = A.step_b.shape[0]
    inner = heads * HEAD
    conv_dim = A.taps.shape[1]
    pre_rows = rows * 2 * A.s_gate.shape[1] // 128
    mine = rows * nz
    dt, gt = depth // 128, inner // 128
    state_shape = A.state.shape
    A.state = A.state.reshape(rows * gt, 128, STATE)
    A.write, A.read, A.step_w, A.out_w, A.router = A.write.T, A.read.T, A.step_w.T, A.out_w.T, A.router.T
    A.mgain, A.fgain = A.mgain.reshape(dt, 128), A.fgain.reshape(dt, 128)
    A.step_b, A.dlog, A.skip = A.step_b.reshape(1, heads), A.dlog.reshape(1, heads), A.skip.reshape(1, heads)
    A.cbias, A.ggain = A.cbias.reshape(1, conv_dim), A.ggain.reshape(1, inner)

    def like(array, *lead):
        return pltpu.VMEM((*lead, *array.shape), array.dtype)

    def f32(*shape):
        return pltpu.VMEM(shape, F32)

    def bf16(*shape):
        return pltpu.VMEM(shape, BF16)

    def sems(n):
        return pltpu.SemaphoreType.DMA((n,))

    scratch = dict(
        v_hidden=like(A.hidden), v_mgain=like(A.mgain), v_step_w=like(A.step_w), v_step_b=like(A.step_b), v_dlog=like(A.dlog),
        v_dshift=like(A.dshift), v_skip=like(A.skip), v_ids=like(A.ids), v_taps=like(A.taps), v_cbias=like(A.cbias),
        v_window=like(A.window), v_ggain=like(A.ggain), v_fgain=like(A.fgain), v_router=like(A.router), v_s_down=like(A.s_down),
        wg=like(A.gate, 2), wi=like(A.input, 2), wwr=like(A.write, 4), wo=like(A.out_w, 2), sg=like(A.s_gate, 2),
        su=like(A.s_up, 2), eg=like(A.e_gate[0], 2), eu=like(A.e_up[0], 2), ed=like(A.e_down[0], 2),
        t1=f32(rows * dt, 128), t2=f32(8, heads), t3=f32(rows * gt, 128), t6=f32(pre_rows, 128), ex=f32(8, inner),
        dcol=f32(rows, heads, STATE), conv=f32(rows, conv_dim), nwf=f32(rows, 3, conv_dim),
        sbf=bf16(rows * gt, 128, STATE), f1=f32(mine * 24, 128), f3=f32(mine * 40, 128), m5=f32(mine * 24, 128),
        m6=f32(nz * pre_rows, 128), hcol=f32(mine, 128), ut=bf16(rows, 128, 128), wt=f32(rows, 128, STATE), x=bf16(mine, depth), a=bf16(mine, inner), prj=f32(5, mine, 128),
        m=f32(nz * 16, 128), member=f32(mine, 128), u2=f32(rows * gt, 128), w2=f32(rows * GROUPS, 128),
        hid_e=bf16(2, mine, A.e_gate.shape[2]), squares=f32(mine, 128), logits=f32(mine, A.router.shape[0]),
        pre=f32(4, mine, A.e_gate.shape[2]),
        hbuf=bf16(nz, rows * dt, 128), gbuf=bf16(nz, rows * gt, 128), rbuf=bf16(nz, mine, 128), pout=bf16(nz, 16, 128),
        pin=bf16(nz, 16, 128), qout=bf16(nz, pre_rows, 128), qmid=bf16(nz, pre_rows, 128), qfin=bf16(nz, pre_rows, 128), cout=bf16(nz, rows * dt, 128),
        cmid=bf16(nz, rows * dt, 128), cfin=bf16(nz, rows * dt, 128),
        load_sem=sems(26), swap_s=sems(10), swap_r=sems(10), h_r=sems(3), g_r=sems(7), r_r=sems(nz - 1), one=sems(5), q_sem=sems(4), c_sem=sems(4),
    )
    outs = dict(o_out=like(A.hidden), o_state=like(A.state), o_window=like(A.window))
    vm, anywhere = pl.BlockSpec(memory_space=pltpu.VMEM), pl.BlockSpec(memory_space=pl.ANY)
    made = pl.pallas_call(
        functools.partial(kernel, nz, rows, inputs + tuple(outs) + tuple(scratch)),
        out_shape=tuple(outs.values()),
        in_specs=[anywhere] * len(inputs),
        out_specs=(vm,) * 3,
        scratch_shapes=list(scratch.values()),
        compiler_params=pltpu.CompilerParams(collective_id=0, has_side_effects=True, vmem_limit_bytes=48 * 1024 * 1024),
        name="layer",
    )(*[getattr(A, name) for name in inputs])
    out, state, window = pl.pallas_call(
        write_out,
        out_shape=tuple(jax.ShapeDtypeStruct(v.shape, v.dtype) for v in made),
        in_specs=[vm] * 3,
        out_specs=(anywhere,) * 3,
        scratch_shapes=[sems(2 + PIECES)],
        compiler_params=pltpu.CompilerParams(vmem_limit_bytes=2**20),
        name="store",
    )(*[pltpu.with_memory_space_constraint(v, pltpu.VMEM) for v in made])
    return out, state.reshape(state_shape), window


PIECES = 4


def write_out(x, state, window, o_x, o_state, o_window, sem):
    copies = []
    step = state.shape[0] // PIECES
    for i in range(PIECES):
        copies.append(pltpu.make_async_copy(state.at[pl.ds(i * step, step)], o_state.at[pl.ds(i * step, step)], sem.at[i]))
    copies.append(pltpu.make_async_copy(x, o_x, sem.at[PIECES]))
    copies.append(pltpu.make_async_copy(window, o_window, sem.at[PIECES + 1]))
    for copy in copies:
        copy.start()
    for copy in copies:
        copy.wait()


def solution(mesh):
    nz = mesh.shape["ep"] // 2
    rows2, rows3, rows4 = P(GRP_EP, None), P(GRP_EP, None, None), P(GRP_EP, None, None, None)
    cols, lead, lead3 = P(None, "ep"), P("ep", None), P("ep", None, None)
    return jax.shard_map(
        functools.partial(layer, nz),
        mesh=mesh,
        in_specs=(
            rows2, rows3, rows4, cols, cols, cols, cols, P(), P(), P(), rows2, P(), P(), P(), P(), P(), cols, P(), P(), rows2,
            lead3, lead3, lead3, lead, lead, P(),
        ),
        out_specs=(rows2, rows4, rows3),
        check_vma=False,
    )
```
